256 devices in a mesh: sp: 16 (over y, x), tp: 16 (over z, core).
Axes of the slice: x: 4, y: 4, z: 8, core: 2. Of those that a mesh axis runs over, the one named last changes fastest.
Arguments:
- saved_input: bfloat16 [4096, 2048], P('sp'), may hold values from -6 to 6
- cotangent: bfloat16 [4096, 2048], P('sp'), may hold values from -6 to 6
- expert_ids: int32 [4096, 2], P('sp'), may hold values from 0 to 15, all different within a row; in each aligned block of 256 rows (0 to 255, 256 to 511, ...) at most 64 rows name the same one
- route_weight: float32 [4096, 2], P('sp'), may hold values from 0.1 to 0.9
- w_gate: bfloat16 [16, 2048, 6144], P('sp', None, 'tp'), may hold values from -0.125 to 0.125
- w_up: bfloat16 [16, 2048, 6144], P('sp', None, 'tp'), may hold values from -0.125 to 0.125
- w_down: bfloat16 [16, 6144, 2048], P('sp', 'tp'), may hold values from -0.078125 to 0.078125
- w_out: bfloat16 [2048, 2048], P(None, 'tp'), may hold values from -0.125 to 0.125
- channel_gain: float32 [2048], P('tp'), may hold values from 0.1 to 1.9
- conv_taps: float32 [31, 2048], P(None, 'tp'), may hold values from -1 to 1
- glu_value: bfloat16 [2048, 4096], P('tp', 'sp'), may hold values from -6 to 6
- glu_gate: bfloat16 [2048, 4096], P('tp', 'sp'), may hold values from -8 to 8
- conv_out: bfloat16 [2048, 4096], P('tp', 'sp'), may hold values from -6 to 6
- norm_mean: float32 [4096], P('sp'), may hold values from -3 to 3
- norm_rstd: float32 [4096], P('sp'), may hold values from 0.5 to 2
Outputs:
- gate_grad: bfloat16 [16, 2048, 6144], P('sp', None, 'tp')
- up_grad: bfloat16 [16, 2048, 6144], P('sp', None, 'tp')
- down_grad: bfloat16 [16, 6144, 2048], P('sp', 'tp')
- proj_grad: float32 [2048, 2048], P('sp', 'tp')
- value_grad: bfloat16 [2048, 4096], P('tp', 'sp')
- gate_in_grad: bfloat16 [2048, 4096], P('tp', 'sp')
The draws below stay inside these ranges and needn't reach their ends.
Inputs may be any that keep to these rules, and one draw needn't show every extreme that they name: `expert_ids`: the two experts of a position differ. In the positions of one block of 256, no expert is named more than 64 times, a bound that some block reaches.
All inputs are finite; a program needn't handle non-finite values.
Results may differ from the reference program's by a relative error of at most 0.018.
Values may be sent and summed in bfloat16 or wider, within the bound.
A program may use at most 128 MiB of HBM per device.

```python
import math
import jax
import jax.numpy as jnp
import numpy as np
from jax import lax

D = 2048
C = 2048
FF = 6144
CONV_K = 31
TOK_SP = 256
EXPERTS = 16
TOKENS = 4096
CAP = 64
N_SP = 16


def strengthened(drawn, key, source, target, blocks, factor):
    owner, partner = [(jnp.arange(drawn.shape[dim]) // (drawn.shape[dim] // blocks)).reshape([-1 if axis == dim else 1 for axis in range(drawn.ndim)]) for dim in (source, target)]
    chosen = jax.random.permutation(key, blocks)[partner]
    strong = (owner == chosen) | (owner == (partner + blocks // 2) % blocks)
    return jnp.where(strong, factor * drawn, drawn)


def levels(stream_key, dims, split, least, high):
    level = 1.0
    for position, blocks in split:
        heights = jax.random.uniform(jax.random.fold_in(jax.random.fold_in(stream_key, 6), position), (blocks,), jnp.float32, least / len(split), high / len(split))
        level = level * jnp.repeat(jnp.exp(heights), dims[position] // blocks).reshape((-1,) + (1,) * (len(dims) - 1 - position))
    return level


def shared_out(key, own, number, rows, amount, top, bound, skew):
    sequence = jax.random.permutation(key, amount)
    crowded, usual = portions_of(amount, rows * top, bound, skew, True), portions_of(amount, rows * top, bound, skew, False)
    places = jnp.arange(amount)

    def named(tallies, rotation):
        used = int((tallies > 0).sum())
        fixed = max(1, used // 4)
        shifted = fixed + (places - fixed + rotation * (used - fixed)) % max(1, amount - fixed)
        return jnp.zeros((amount,), jnp.int32).at[sequence[jnp.where(places < fixed, places, shifted)]].set(jnp.asarray(tallies, jnp.int32))

    tallies = jnp.where(number % 4 == 0, named(crowded, number // 4), named(usual, number - number // 4 - 1))
    mixed = jax.random.permutation(jax.random.fold_in(own, 3), amount)
    giver, taker = mixed[0:amount // 2 * 2:2], mixed[1:amount // 2 * 2:2]
    room = jnp.minimum(tallies[giver] - 1, bound - tallies[taker]) // 2
    room = jnp.where((giver == sequence[0]) | (taker == sequence[0]) | (tallies[taker] == 0), 0, jnp.maximum(room, 0))
    shifted = jax.random.randint(jax.random.fold_in(own, 4), (amount // 2,), 0, 1 << 20) % (room + 1)
    tallies = tallies.at[giver].add(-shifted).at[taker].add(shifted)
    items = jnp.searchsorted(jnp.cumsum(tallies), jnp.arange(rows * top), side="right").astype(jnp.int32)
    grid = items.reshape(top, rows).T
    grid = grid[jax.random.permutation(jax.random.fold_in(own, 1), rows)]
    rotation = jax.random.randint(jax.random.fold_in(own, 2), (rows, 1), 0, top)
    return jnp.take_along_axis(grid, (jnp.arange(top)[None, :] + rotation) % top, axis=1)


def portions_of(number_of, total, most, lean, full):
    loads = [(1 << 20) // math.isqrt(standing ** lean) + 1 for standing in range(1, number_of + 1)]
    largest = most if full else min(most, max(-(-total // number_of), total * loads[0] // sum(loads)))
    least = 1 if total - largest >= number_of - 1 else 0
    given, rest = [largest] + [least] * (number_of - 1), total - largest - least * (number_of - 1)
    while rest > 0:
        movable = [i for i in range(1, number_of) if given[i] < largest] or [i for i in range(1, number_of) if given[i] < most]
        whole, budget = sum([loads[i] for i in movable]), rest
        for i in movable:
            addition = min(most - given[i], max(1, budget * loads[i] // whole), rest)
            given[i] = given[i] + addition
            rest = rest - addition
    return np.array(given)


def gaussian(stream_key, dims, deviation, reach, pieces=(), held_as=jnp.bfloat16):
    factor_of = levels(stream_key, dims, pieces, -0.22, 0.18) if pieces else 1.0
    result = jax.random.normal(stream_key, dims, jnp.float32) * deviation * factor_of
    return jnp.minimum(jnp.maximum(result, -reach), reach).astype(held_as)


def bell_draw_with(key, extent, scale, reach, shards, heavy, held_as=jnp.bfloat16):
    drawn = scale * jax.random.normal(key, extent, jnp.float32)
    if shards:
        drawn = drawn * levels(key, extent, shards, -0.22, 0.18)
    return jnp.clip(strengthened(drawn, jax.random.fold_in(key, 3), *heavy), -reach, reach).astype(held_as)


def setup_inputs(seed: int = 0) -> dict:
    key_list = jax.random.split(jax.random.key(seed), 16)
    saved_input = gaussian(key_list[0], (TOKENS, D), 1.0, 6.0, ((0, 16),))
    cotangent = bell_draw_with(key_list[1], (TOKENS, D), 1.0, 6.0, ((0, 16),), (0, 1, 16, 2.0))
    expert_ids_keys = jax.random.split(jax.random.fold_in(key_list[2], 1), TOKENS // TOK_SP)
    expert_ids_turns = jax.random.permutation(jax.random.fold_in(key_list[2], 3), TOKENS // TOK_SP)
    expert_ids = jax.vmap(lambda own, number: shared_out(jax.random.fold_in(key_list[2], 2), own, number, TOK_SP, EXPERTS, 2, CAP, 1))(expert_ids_keys, expert_ids_turns).reshape((TOKENS, 2))
    route_weight = jnp.clip(0.1 + 0.79999997 * jax.random.uniform(key_list[3], (TOKENS, 2), jnp.float32) ** levels(key_list[3], (TOKENS, 2), ((0, 16),), -0.2, 0.2), 0.1, 0.9)
    w_gate = gaussian(key_list[4], (EXPERTS, D, FF), D ** -0.5, 0.125, ((0, 16), (2, 16)))
    w_up = gaussian(key_list[5], (EXPERTS, D, FF), D ** -0.5, 0.125, ((0, 16), (2, 16)))
    w_down = gaussian(key_list[6], (EXPERTS, FF, D), FF ** -0.5, 0.078125, ((0, 16), (1, 16)))
    w_out = gaussian(key_list[7], (D, C), C ** -0.5, 0.125, ((1, 16),))
    channel_gain = jnp.clip(1.0 + 0.18 * jax.random.normal(key_list[8], (C,), jnp.float32), 0.1, 1.9)
    conv_taps = gaussian(key_list[9], (CONV_K, C), CONV_K ** -0.5, 1.0, ((1, 16),), jnp.float32)
    glu_value = gaussian(key_list[10], (C, TOKENS), 1.0, 6.0, ((0, 16), (1, 16)))
    glu_gate = gaussian(key_list[11], (C, TOKENS), 1.5, 8.0, ((0, 16), (1, 16)))
    conv_out = gaussian(key_list[12], (C, TOKENS), 1.0, 6.0, ((0, 16), (1, 16)))
    norm_mean = gaussian(key_list[13], (TOKENS,), 0.5, 3.0, ((0, 16),), jnp.float32)
    norm_rstd = jnp.clip(jnp.exp(math.log(2.0) - 1.3862944 * jax.random.uniform(key_list[14], (TOKENS,), jnp.float32) ** levels(key_list[14], (TOKENS,), ((0, 16),), -0.2, 0.2)), 0.5, 2.0)
    return dict(saved_input=saved_input, cotangent=cotangent, expert_ids=expert_ids, route_weight=route_weight, w_gate=w_gate, w_up=w_up, w_down=w_down, w_out=w_out, channel_gain=channel_gain, conv_taps=conv_taps, glu_value=glu_value, glu_gate=glu_gate, conv_out=conv_out, norm_mean=norm_mean, norm_rstd=norm_rstd)


def contract(left, right, left_dim, right_dim):
    return lax.dot_general(left, right, (((left_dim,), (right_dim,)), ((), ())), preferred_element_type=jnp.float32)


def expert_grads(rows_in, rows_cot, gate_weight, up_weight, down_weight):
    gate_pre = jnp.dot(rows_in, gate_weight, preferred_element_type=jnp.float32)
    up_pre = jnp.dot(rows_in, up_weight, preferred_element_type=jnp.float32)
    sigma = jax.nn.sigmoid(gate_pre)
    hidden = (gate_pre * sigma * up_pre).astype(jnp.bfloat16)
    hidden_cot = contract(rows_cot, down_weight, 1, 1)
    down_part = contract(hidden, rows_cot, 0, 0).astype(jnp.bfloat16)
    gate_cot = (hidden_cot * up_pre * sigma * (1.0 + gate_pre * (1.0 - sigma))).astype(jnp.bfloat16)
    up_cot = (hidden_cot * gate_pre * sigma).astype(jnp.bfloat16)
    gate_part = contract(rows_in, gate_cot, 0, 0).astype(jnp.bfloat16)
    up_part = contract(rows_in, up_cot, 0, 0).astype(jnp.bfloat16)
    input_cot = contract(gate_cot, gate_weight, 1, 1) + contract(up_cot, up_weight, 1, 1)
    return gate_part, up_part, down_part, input_cot


def reference(saved_input, cotangent, expert_ids, route_weight, w_gate, w_up, w_down, w_out,
              channel_gain, conv_taps, glu_value, glu_gate, conv_out, norm_mean, norm_rstd):
    pairs = expert_ids.reshape(N_SP, 2 * TOK_SP)
    onehot = (pairs[:, :, None] == jnp.arange(EXPERTS, dtype=jnp.int32)[None, None, :]).astype(jnp.int32)
    before = jnp.cumsum(onehot, axis=1) - onehot
    slots = jnp.sum(before * onehot, axis=2)
    source = jnp.arange(N_SP, dtype=jnp.int32)[:, None]
    target = (pairs * (N_SP * CAP) + source * CAP + slots).reshape(2 * TOKENS).astype(jnp.int32)
    owner = jnp.zeros((EXPERTS * N_SP * CAP,), jnp.int32).at[target].set(jnp.arange(2 * TOKENS, dtype=jnp.int32) + 1)
    filled = (owner > 0)[:, None]
    pair_index = jnp.maximum(owner - 1, 0)
    scaled = (route_weight[:, :, None] * cotangent.astype(jnp.float32)[:, None, :]).astype(jnp.bfloat16)
    scaled = scaled.reshape(2 * TOKENS, D)
    rows_cot = jnp.where(filled, scaled[pair_index], jnp.zeros_like(scaled[:1])).reshape(EXPERTS, N_SP * CAP, D)
    rows_in = jnp.where(filled, saved_input[pair_index // 2], jnp.zeros_like(saved_input[:1]))
    rows_in = rows_in.reshape(EXPERTS, N_SP * CAP, D)
    gate_grad, up_grad, down_grad, input_cot = lax.map(
        lambda packed: expert_grads(*packed), (rows_in, rows_cot, w_gate, w_up, w_down))
    routed = input_cot.reshape(EXPERTS * N_SP * CAP, D)[target].reshape(TOKENS, 2, D)
    mixed_cot = (cotangent.astype(jnp.float32) + jnp.sum(routed, axis=1)).astype(jnp.bfloat16)

    centered = (conv_out.astype(jnp.float32) - norm_mean[None, :]) * norm_rstd[None, :]
    normed = centered * channel_gain[:, None]
    sigma = jax.nn.sigmoid(normed)
    output_act = (normed * sigma).astype(jnp.bfloat16)
    proj_grad = contract(mixed_cot, output_act, 0, 1)
    act_cot = contract(w_out, mixed_cot, 0, 1)
    norm_cot = act_cot * sigma * (1.0 + normed * (1.0 - sigma)) * channel_gain[:, None]
    first_sum = jnp.sum(norm_cot, axis=0)
    second_sum = jnp.sum(norm_cot * centered, axis=0)
    conv_cot = norm_rstd[None, :] * (norm_cot - first_sum[None, :] / C - centered * second_sum[None, :] / C)
    padded = jnp.pad(conv_cot, ((0, 0), (0, CONV_K - 1)))
    glu_cot = conv_taps[0][:, None] * padded[:, :TOKENS]
    for lag in range(1, CONV_K):
        glu_cot = glu_cot + conv_taps[lag][:, None] * padded[:, lag:lag + TOKENS]
    gate_sigma = jax.nn.sigmoid(glu_gate.astype(jnp.float32))
    value_grad = (glu_cot * gate_sigma).astype(jnp.bfloat16)
    gate_in_grad = (glu_cot * glu_value.astype(jnp.float32) * gate_sigma * (1.0 - gate_sigma)).astype(jnp.bfloat16)
    return gate_grad, up_grad, down_grad, proj_grad, value_grad, gate_in_grad
```

```python
import functools

import jax
import jax.numpy as jnp
from jax import lax
from jax.experimental import pallas as pl
from jax.experimental.pallas import tpu as pltpu
from jax.sharding import PartitionSpec as P

D = 2048
C = 2048
SIDE = 4
RING = 8
CAP = 64
BF16 = jnp.bfloat16
F32 = jnp.float32
MESH = pl.DeviceIdType.MESH

FAR = ((0, 2), (2, 0), (1, 2), (3, 2), (2, 1), (2, 3), (2, 2))
NEAR = ((0, 1), (0, 3), (1, 0), (3, 0), (1, 1), (1, 3), (3, 1), (3, 3))
OFFSETS = FAR + NEAR + ((0, 0),)
HALVES = ((0, 4), (4, 3))


def sp_at(dy, dx):
    sp = lax.axis_index("sp")
    y, x = sp // SIDE, sp % SIDE
    return ((y + dy) % SIDE) * SIDE + (x + dx) % SIDE


def contract(left, right, left_dim, right_dim):
    return lax.dot_general(
        left, right, (((left_dim,), (right_dim,)), ((), ())), preferred_element_type=F32
    )


def greet(others):
    barrier = pltpu.get_barrier_semaphore()
    for device in others:
        pl.semaphore_signal(barrier, inc=1, device_id=device, device_id_type=MESH)
    pl.semaphore_wait(barrier, len(others))


def group(with_sp):
    sp, tp = lax.axis_index("sp"), lax.axis_index("tp")
    z, core = tp // 2, tp % 2
    partner = (sp, z * 2 + 1 - core)
    up = (sp, ((z + 1) % RING) * 2 + core)
    down = (sp, ((z + RING - 1) % RING) * 2 + core)
    others = [partner, up, down]
    if with_sp:
        others += [(sp_at(dy, dx), tp) for dy, dx in OFFSETS[:-1]]
    return sp, tp, z, core, partner, up, down, others


class Copies:
    def __init__(self):
        self.started = []

    def send(self, src, dst, send_sem, recv_sem, device):
        copy = pltpu.make_async_remote_copy(
            src_ref=src,
            dst_ref=dst,
            send_sem=send_sem,
            recv_sem=recv_sem,
            device_id=device,
            device_id_type=MESH,
        )
        copy.start()
        self.started.append(copy)

    def arrived(self, dst, send_sem, recv_sem, device):
        pltpu.make_async_remote_copy(
            src_ref=dst,
            dst_ref=dst,
            send_sem=send_sem,
            recv_sem=recv_sem,
            device_id=device,
            device_id_type=MESH,
        ).wait_recv()

    def finish(self):
        for copy in self.started:
            copy.wait_send()


def select_kernel(ids_ref, weight_ref, in_ref, cot_ref, x_ref, row_ref, src0, src1):
    core = lax.axis_index("tp") % 2
    sp = lax.axis_index("sp")
    y, x = sp // SIDE, sp % SIDE
    tokens = in_ref.shape[0]
    lanes = lax.broadcasted_iota(jnp.int32, (tokens, 128), 1)
    one = [(ids_ref[:, k : k + 1] == lanes).astype(F32) for k in range(2)]
    count = (one[0] + one[1]).astype(BF16)
    earlier = (
        lax.broadcasted_iota(jnp.int32, (tokens, tokens), 0)
        > lax.broadcasted_iota(jnp.int32, (tokens, tokens), 1)
    ).astype(BF16)
    before = jnp.dot(earlier, count, preferred_element_type=F32)
    place = jnp.zeros((1, 128), jnp.int32)
    lane = lax.broadcasted_iota(jnp.int32, (1, 128), 1)
    for o, (dy, dx) in enumerate(OFFSETS):
        expert = ((y + dy) % SIDE) * SIDE + (x + dx) % SIDE
        place = jnp.where(lane == expert, o * CAP, place)
    row_of = before + place.astype(F32)
    rows = [
        jnp.sum(one[k] * row_of, axis=1, keepdims=True).astype(jnp.int32) for k in range(2)
    ]
    for k in range(2):
        row_ref[:, k : k + 1] = rows[k]
    cot = cot_ref[...].astype(F32)
    for k, src in enumerate((src0, src1)):
        scaled = (weight_ref[:, k : k + 1] * cot).astype(BF16)
        src[...] = jnp.where(core == 0, in_ref[...], scaled)

    def step(o, carry):
        at = lax.broadcasted_iota(jnp.int32, (tokens, 2 * CAP), 1) + o * (2 * CAP)
        total = contract((rows[0] == at).astype(BF16), src0[...], 0, 0) + contract(
            (rows[1] == at).astype(BF16), src1[...], 0, 0
        )
        x_ref[pl.ds(2 * o, 2)] = total.astype(BF16).reshape(2, RING, 8, D)
        return carry

    lax.fori_loop(0, len(OFFSETS) // 2, step, 0)


def select(ids, weight, rows_in, rows_cot):
    tokens = rows_in.shape[0]
    vmem = pl.BlockSpec(memory_space=pltpu.VMEM)
    return pl.pallas_call(
        select_kernel,
        out_shape=(
            jax.ShapeDtypeStruct((len(OFFSETS), RING, 8, D), BF16),
            jax.ShapeDtypeStruct((tokens, 2), jnp.int32),
        ),
        in_specs=[vmem] * 4,
        out_specs=(vmem, vmem),
        scratch_shapes=[pltpu.VMEM((tokens, D), BF16)] * 2,
        compiler_params=pltpu.CompilerParams(vmem_limit_bytes=24 << 20),
        name="select",
    )(ids, weight, rows_in, rows_cot)


def dispatch_kernel(
    x_ref,
    r_ref,
    far_send,
    far_recv,
    near_send,
    near_recv,
    up_send,
    up_recv,
    down_send,
    down_recv,
    share_send,
    share_recv,
    near_share_send,
    near_share_recv,
    local_sem,
):
    sp, tp, z, core, partner, up, down, others = group(True)
    copies = Copies()
    near_at = len(FAR)
    local_at = len(OFFSETS) - 1
    greet(others)

    def far(c, g, half):
        start, size = HALVES[half]
        return r_ref.at[c, pl.ds(start, size), g]

    for half, (start, size) in enumerate(HALVES):
        for o in range(start, start + size):
            copies.send(
                x_ref.at[o, z],
                r_ref.at[core, o, z],
                far_send.at[o],
                far_recv.at[o],
                (sp_at(*FAR[o]), tp),
            )
    for i, offset in enumerate(NEAR):
        copies.send(
            x_ref.at[near_at + i],
            r_ref.at[core, near_at + i],
            near_send.at[i],
            near_recv.at[i],
            (sp_at(*offset), tp),
        )
    n_near = len(NEAR)
    copies.send(
        x_ref.at[local_at],
        r_ref.at[core, local_at],
        near_share_send.at[n_near],
        near_share_recv.at[n_near],
        partner,
    )
    local = pltpu.make_async_copy(x_ref.at[local_at], r_ref.at[core, local_at], local_sem)
    local.start()

    def spread(g, k, half, going_up, going_down, slot):
        block = far(core, g, half)
        if going_up:
            copies.send(block, block, up_send.at[k, half], up_recv.at[k, half], up)
        if going_down:
            copies.send(block, block, down_send.at[k, half], down_recv.at[k, half], down)
        copies.send(block, block, share_send.at[slot, half], share_recv.at[slot, half], partner)

    for half, (start, size) in enumerate(HALVES):
        for o in range(start, start + size):
            copies.arrived(r_ref.at[core, o, z], far_send.at[o], far_recv.at[o], partner)
        spread(z, 0, half, True, True, 0)

    for k in range(1, 5):
        above, below = (z + RING - k) % RING, (z + k) % RING
        for half in range(2):
            if k < 4 or half == 0:
                copies.arrived(
                    far(core, above, half), up_send.at[k - 1, half], up_recv.at[k - 1, half], up
                )
                spread(above, k, half, k < 3 or (k == 3 and half == 0), False, k)
            if k < 4 or half == 1:
                copies.arrived(
                    far(core, below, half),
                    down_send.at[k - 1, half],
                    down_recv.at[k - 1, half],
                    down,
                )
                spread(below, k, half, False, k < 3 or (k == 3 and half == 1), 4 if k == 4 else 4 + k)
        for i in (2 * k - 2, 2 * k - 1):
            block = r_ref.at[core, near_at + i]
            copies.arrived(block, near_send.at[i], near_recv.at[i], partner)
            copies.send(block, block, near_share_send.at[i], near_share_recv.at[i], partner)

    for slot in range(RING):
        g = (z + RING - slot) % RING if slot <= 4 else (z + slot - 4) % RING
        for half in range(2):
            copies.arrived(
                far(1 - core, g, half),
                share_send.at[slot, half],
                share_recv.at[slot, half],
                partner,
            )
    for i in range(n_near + 1):
        copies.arrived(
            r_ref.at[1 - core, near_at + i], near_share_send.at[i], near_share_recv.at[i], partner
        )
    local.wait()
    copies.finish()


def dispatch(x):
    dma = pltpu.SemaphoreType.DMA
    n_near = len(NEAR)
    return pl.pallas_call(
        dispatch_kernel,
        out_shape=jax.ShapeDtypeStruct((2, *x.shape), BF16),
        in_specs=[pl.BlockSpec(memory_space=pltpu.VMEM)],
        out_specs=pl.BlockSpec(memory_space=pl.ANY),
        scratch_shapes=[
            dma((len(FAR),)),
            dma((len(FAR),)),
            dma((n_near,)),
            dma((n_near,)),
            dma((4, 2)),
            dma((4, 2)),
            dma((4, 2)),
            dma((4, 2)),
            dma((RING, 2)),
            dma((RING, 2)),
            dma((n_near + 1,)),
            dma((n_near + 1,)),
            dma,
        ],
        compiler_params=pltpu.CompilerParams(
            collective_id=0, has_side_effects=True, vmem_limit_bytes=24 << 20
        ),
        name="dispatch",
    )(x)


def input_kernel(gate_ref, up_ref, wg_ref, wu_ref, out_ref):
    total = contract(gate_ref[...], wg_ref[...], 1, 1) + contract(up_ref[...], wu_ref[...], 1, 1)
    total = total.astype(BF16)
    out_ref[0, 0] = total[:, :128]
    out_ref[1, 0] = total[:, 128:]


def input_shares(gate_cot, up_cot, w_gate, w_up):
    rows, hidden = gate_cot.shape
    whole = pl.BlockSpec((rows, hidden), lambda i: (0, 0))
    part = pl.BlockSpec((256, hidden), lambda i: (i, 0))
    return pl.pallas_call(
        input_kernel,
        grid=(RING,),
        out_shape=jax.ShapeDtypeStruct((2, RING, rows, 128), BF16),
        in_specs=[whole, whole, part, part],
        out_specs=pl.BlockSpec((2, 1, rows, 128), lambda i: (0, i, 0, 0)),
        compiler_params=pltpu.CompilerParams(vmem_limit_bytes=24 << 20),
        name="input_shares",
    )(gate_cot, up_cot, w_gate, w_up)


def collect_kernel(
    p_ref,
    row_ref,
    cot_ref,
    m_ref,
    pair_buf,
    out_up,
    in_up,
    out_down,
    in_down,
    sums,
    slots,
    cot_buf,
    mixed,
    pair_send,
    pair_recv,
    up_send,
    up_recv,
    down_send,
    down_recv,
    back_send,
    back_recv,
    gup_send,
    gup_recv,
    gdown_send,
    gdown_recv,
    share_send,
    share_recv,
    local_sem,
):
    sp, tp, z, core, partner, up, down, others = group(True)
    rows = p_ref.shape[2]
    tokens = m_ref.shape[0]
    half_rows = rows // 2
    half_tokens = tokens // 2
    copies = Copies()
    greet(others)
    order = (4, 3, -3, 2, -2, 1, -1, 0)
    for i, d in enumerate(order):
        g = (z + RING + d) % RING
        copies.send(
            p_ref.at[1 - core, g], pair_buf.at[g], pair_send.at[i], pair_recv.at[i], partner
        )
    fetch = pltpu.make_async_copy(
        cot_ref.at[:, pl.ds(pl.multiple_of(tp * 128, 128), 128)], cot_buf, local_sem.at[0]
    )
    fetch.start()

    def paired(d):
        i = order.index(d)
        g = (z + RING + d) % RING
        copies.arrived(pair_buf.at[g], pair_send.at[i], pair_recv.at[i], partner)

    def span(half):
        return pl.ds(half * half_rows, half_rows)

    def own(d, half):
        g = (z + RING + d) % RING
        return p_ref[core, g, span(half), :].astype(F32) + pair_buf[g, span(half), :].astype(F32)

    def go_up(hop, half):
        copies.send(
            out_up.at[hop, span(half)],
            in_up.at[hop, span(half)],
            up_send.at[hop, half],
            up_recv.at[hop, half],
            up,
        )

    def go_down(hop, half):
        copies.send(
            out_down.at[hop, span(half)],
            in_down.at[hop, span(half)],
            down_send.at[hop, half],
            down_recv.at[hop, half],
            down,
        )

    def from_up(hop, half):
        copies.arrived(
            in_up.at[hop, span(half)], up_send.at[hop, half], up_recv.at[hop, half], up
        )
        return in_up[hop, span(half), :].astype(F32)

    def from_down(hop, half):
        copies.arrived(
            in_down.at[hop, span(half)], down_send.at[hop, half], down_recv.at[hop, half], down
        )
        return in_down[hop, span(half), :].astype(F32)

    paired(4)
    out_up[0, span(0), :] = own(4, 0).astype(BF16)
    out_down[0, span(1), :] = own(-4, 1).astype(BF16)
    go_up(0, 0)
    go_down(0, 1)
    paired(3)
    paired(-3)
    out_up[1, span(1), :] = own(3, 1).astype(BF16)
    out_down[1, span(0), :] = own(-3, 0).astype(BF16)
    go_up(1, 1)
    go_down(1, 0)
    for hop in range(1, 4):
        d = 4 - hop
        if hop > 1:
            paired(d)
            paired(-d)
        out_up[hop, span(0), :] = (from_up(hop - 1, 0) + own(d, 0)).astype(BF16)
        out_down[hop, span(1), :] = (from_down(hop - 1, 1) + own(-d, 1)).astype(BF16)
        go_up(hop, 0)
        go_down(hop, 1)
        if hop > 1:
            out_up[hop, span(1), :] = (from_up(hop - 1, 1) + own(d, 1)).astype(BF16)
            out_down[hop, span(0), :] = (from_down(hop - 1, 0) + own(-d, 0)).astype(BF16)
            go_up(hop, 1)
            go_down(hop, 0)
    paired(0)
    for half in range(2):
        sums[span(half), :] = (
            own(0, half) + from_up(3, half) + from_down(3, half)
        ).astype(BF16)
    for o, (dy, dx) in enumerate(OFFSETS[:-1]):
        part = pl.ds(o * CAP, CAP)
        copies.send(
            sums.at[part],
            slots.at[part],
            back_send.at[o],
            back_recv.at[o],
            (sp_at(-dy, -dx), tp),
        )
    here = pl.ds((len(OFFSETS) - 1) * CAP, CAP)
    slots[here, :] = sums[here, :]
    at = lax.broadcasted_iota(jnp.int32, (tokens, rows), 1)
    chosen = ((row_ref[:, 0:1] == at) | (row_ref[:, 1:2] == at)).astype(BF16)
    fetch.wait()
    for o in range(len(OFFSETS) - 1):
        copies.arrived(slots.at[pl.ds(o * CAP, CAP)], back_send.at[o], back_recv.at[o], partner)
    total = jnp.dot(chosen, slots[...], preferred_element_type=F32)
    mixed[...] = (cot_buf[...].astype(F32) + total).astype(BF16)

    def block(g, c, half):
        return m_ref.at[
            pl.ds(half * half_tokens, half_tokens),
            pl.ds(pl.multiple_of((g * 2 + c) * 128, 128), 128),
        ]

    def spread(src, g, k, half, going_up, going_down, slot):
        dst = block(g, core, half)
        if going_up:
            copies.send(src, dst, gup_send.at[k, half], gup_recv.at[k, half], up)
        if going_down:
            copies.send(src, dst, gdown_send.at[k, half], gdown_recv.at[k, half], down)
        copies.send(src, dst, share_send.at[slot, half], share_recv.at[slot, half], partner)

    keep = []
    for half in range(2):
        src = mixed.at[pl.ds(half * half_tokens, half_tokens)]
        spread(src, z, 0, half, True, True, 0)
        copy = pltpu.make_async_copy(src, block(z, core, half), local_sem.at[1 + half])
        copy.start()
        keep.append(copy)
    for k in range(1, 5):
        above, below = (z + RING - k) % RING, (z + k) % RING
        for half in range(2):
            if k < 4 or half == 0:
                dst = block(above, core, half)
                copies.arrived(dst, gup_send.at[k - 1, half], gup_recv.at[k - 1, half], up)
                spread(dst, above, k, half, k < 3 or (k == 3 and half == 0), False, k)
            if k < 4 or half == 1:
                dst = block(below, core, half)
                copies.arrived(dst, gdown_send.at[k - 1, half], gdown_recv.at[k - 1, half], down)
                spread(
                    dst,
                    below,
                    k,
                    half,
                    False,
                    k < 3 or (k == 3 and half == 1),
                    4 if k == 4 else 4 + k,
                )
    for slot in range(RING):
        g = (z + RING - slot) % RING if slot <= 4 else (z + slot - 4) % RING
        for half in range(2):
            copies.arrived(
                block(g, 1 - core, half),
                share_send.at[slot, half],
                share_recv.at[slot, half],
                partner,
            )
    for copy in keep:
        copy.wait()
    copies.finish()


def collect(shares, rows_of, cotangent):
    dma = pltpu.SemaphoreType.DMA
    rows = shares.shape[2]
    tokens = cotangent.shape[0]
    n_back = len(OFFSETS) - 1
    vmem = pl.BlockSpec(memory_space=pltpu.VMEM)
    return pl.pallas_call(
        collect_kernel,
        out_shape=jax.ShapeDtypeStruct((tokens, D), BF16),
        in_specs=[vmem, vmem, pl.BlockSpec(memory_space=pl.ANY)],
        out_specs=vmem,
        scratch_shapes=[
            pltpu.VMEM((RING, rows, 128), BF16),
            pltpu.VMEM((4, rows, 128), BF16),
            pltpu.VMEM((4, rows, 128), BF16),
            pltpu.VMEM((4, rows, 128), BF16),
            pltpu.VMEM((4, rows, 128), BF16),
            pltpu.VMEM((rows, 128), BF16),
            pltpu.VMEM((rows, 128), BF16),
            pltpu.VMEM((tokens, 128), BF16),
            pltpu.VMEM((tokens, 128), BF16),
            dma((RING,)),
            dma((RING,)),
            dma((4, 2)),
            dma((4, 2)),
            dma((4, 2)),
            dma((4, 2)),
            dma((n_back,)),
            dma((n_back,)),
            dma((4, 2)),
            dma((4, 2)),
            dma((4, 2)),
            dma((4, 2)),
            dma((RING, 2)),
            dma((RING, 2)),
            dma((3,)),
        ],
        compiler_params=pltpu.CompilerParams(
            collective_id=1, has_side_effects=True, vmem_limit_bytes=32 << 20
        ),
        name="collect",
    )(shares, rows_of, cotangent)


def cut_along(value, dim, devices):
    before, after = (value.shape[:dim], value.shape[dim + 1 :])
    return jnp.moveaxis(value.reshape(*before, devices, -1, *after), dim, 0)


def sent_and_summed(value, axis, dim):
    devices = lax.axis_size(axis)
    tiles = lax.all_to_all(cut_along(value, dim, devices), axis, 0, 0, tiled=True)
    return jnp.sum(tiles.astype(F32), axis=0)


def of_everyone(value, axis):
    copies = jnp.broadcast_to(value, (lax.axis_size(axis), *value.shape))
    everything = lax.all_to_all(copies, axis, split_axis=0, concat_axis=0, tiled=True)
    return jnp.sum(everything, axis=0)


def from_behind(value, axis, by):
    devices = lax.axis_size(axis)
    pairs = [(i, i + by) for i in range(devices) if 0 <= i + by < devices]
    return lax.ppermute(value, axis, pairs)


def on_device(
    saved_input,
    cotangent,
    expert_ids,
    route_weight,
    w_gate,
    w_up,
    w_down,
    w_out,
    channel_gain,
    conv_taps,
    glu_value,
    glu_gate,
    conv_out,
    norm_mean,
    norm_rstd,
):
    tokens_here = cotangent.shape[0]
    gate_weight, up_weight, down_weight = w_gate[0], w_up[0], w_down[0]
    x, rows_of = select(expert_ids, route_weight, saved_input, cotangent)
    arrived = dispatch(x).reshape(2, len(OFFSETS) * CAP, D)
    rows_in, rows_cot = arrived[0], arrived[1]

    gate_pre = jnp.dot(rows_in, gate_weight, preferred_element_type=F32)
    up_pre = jnp.dot(rows_in, up_weight, preferred_element_type=F32)
    sigma = jax.nn.sigmoid(gate_pre)
    hidden = (gate_pre * sigma * up_pre).astype(BF16)
    hidden_cot = contract(rows_cot, down_weight, 1, 1)
    gate_cot = (hidden_cot * up_pre * sigma * (1.0 + gate_pre * (1.0 - sigma))).astype(BF16)
    up_cot = (hidden_cot * gate_pre * sigma).astype(BF16)
    shares = input_shares(gate_cot, up_cot, gate_weight, up_weight)
    mixed_cot = collect(shares, rows_of, cotangent)
    down_grad = contract(hidden, rows_cot, 0, 0).astype(BF16)[None]
    gate_grad = contract(rows_in, gate_cot, 0, 0).astype(BF16)[None]
    up_grad = contract(rows_in, up_cot, 0, 0).astype(BF16)[None]

    centered = (conv_out.astype(F32) - norm_mean[None, :]) * norm_rstd[None, :]
    normed = centered * channel_gain[:, None]
    sigma = jax.nn.sigmoid(normed)
    output_act = (normed * sigma).astype(BF16)
    proj_grad = sent_and_summed(contract(mixed_cot, output_act, 0, 1).astype(BF16), "sp", 0)
    act_cot = contract(w_out, mixed_cot, 0, 1)
    norm_cot = act_cot * sigma * (1.0 + normed * (1.0 - sigma)) * channel_gain[:, None]
    sums = of_everyone(
        jnp.stack([jnp.sum(norm_cot, axis=0), jnp.sum(norm_cot * centered, axis=0)]), "tp"
    )
    first_sum, second_sum = sums[0], sums[1]
    conv_cot = norm_rstd[None, :] * (
        norm_cot - first_sum[None, :] / C - centered * second_sum[None, :] / C
    )
    reach = conv_taps.shape[0] - 1
    rim = from_behind(conv_cot[:, :reach], "sp", -1)
    padded = jnp.concatenate([conv_cot, rim], axis=1)
    glu_cot = conv_taps[0][:, None] * padded[:, :tokens_here]
    for lag in range(1, reach + 1):
        glu_cot = glu_cot + conv_taps[lag][:, None] * padded[:, lag : lag + tokens_here]
    gate_sigma = jax.nn.sigmoid(glu_gate.astype(F32))
    value_grad = (glu_cot * gate_sigma).astype(BF16)
    gate_in_grad = (glu_cot * glu_value.astype(F32) * gate_sigma * (1.0 - gate_sigma)).astype(BF16)
    return (gate_grad, up_grad, down_grad, proj_grad, value_grad, gate_in_grad)


def solution(mesh):
    in_specs = (
        P("sp", None),
        P("sp", None),
        P("sp", None),
        P("sp", None),
        P("sp", None, "tp"),
        P("sp", None, "tp"),
        P("sp", "tp", None),
        P(None, "tp"),
        P("tp"),
        P(None, "tp"),
        P("tp", "sp"),
        P("tp", "sp"),
        P("tp", "sp"),
        P("sp"),
        P("sp"),
    )
    out_specs = (
        P("sp", None, "tp"),
        P("sp", None, "tp"),
        P("sp", "tp", None),
        P("sp", "tp"),
        P("tp", "sp"),
        P("tp", "sp"),
    )
    return jax.shard_map(
        on_device, mesh=mesh, in_specs=in_specs, out_specs=out_specs, check_vma=False
    )
```

```python
import jax
import jax.numpy as jnp
from jax import lax
from jax.experimental import pallas as pl
from jax.experimental.pallas import tpu as pltpu
from jax.sharding import PartitionSpec as P

D = 2048
C = 2048
HIDDEN = 384
SIDE = 4
RING = 8
CAP = 64
BF16 = jnp.bfloat16
F32 = jnp.float32
MESH = pl.DeviceIdType.MESH

NEXT = ((0, 1), (0, 3), (1, 0), (3, 0))
CORNER = ((1, 1), (3, 3), (1, 3), (3, 1))
HERE = ((0, 0),)
ACROSS = ((0, 2), (2, 0))
FAR = ((1, 2), (3, 2), (2, 1), (2, 3), (2, 2))
OFFSETS = NEXT + CORNER + HERE + ACROSS + FAR
N_OFF = len(OFFSETS)
LOCAL = OFFSETS.index((0, 0))
FAR_AT = N_OFF - len(FAR)
HALVES = ((0, 3), (3, 2))
ROWS = N_OFF * CAP


def sp_at(dy, dx):
    sp = lax.axis_index("sp")
    y, x = sp // SIDE, sp % SIDE
    return ((y + dy) % SIDE) * SIDE + (x + dx) % SIDE


def contract(left, right, left_dim, right_dim):
    return lax.dot_general(
        left, right, (((left_dim,), (right_dim,)), ((), ())), preferred_element_type=F32
    )


class Copies:
    def __init__(self):
        self.started = []

    def send(self, src, dst, sems, at, device):
        copy = pltpu.make_async_remote_copy(
            src_ref=src,
            dst_ref=dst,
            send_sem=sems[0].at[at],
            recv_sem=sems[1].at[at],
            device_id=device,
            device_id_type=MESH,
        )
        copy.start()
        self.started.append(copy)

    def arrived(self, dst, sems, at, device):
        pltpu.make_async_remote_copy(
            src_ref=dst,
            dst_ref=dst,
            send_sem=sems[0].at[at],
            recv_sem=sems[1].at[at],
            device_id=device,
            device_id_type=MESH,
        ).wait_recv()

    def finish(self):
        for copy in self.started:
            copy.wait_send()


def spread_ring(copies, block, source, core, z, up, down, partner, ups, downs, shares, between):
    def spread(src, g, k, half, going_up, going_down, slot):
        dst = block(g, core, half)
        if going_up:
            copies.send(src, dst, ups, (k, half), up)
        if going_down:
            copies.send(src, dst, downs, (k, half), down)
        copies.send(src, dst, shares, (slot, half), partner)

    for half in range(2):
        spread(source(half), z, 0, half, True, True, 0)
    between(0)
    for k in range(1, 5):
        above, below = (z + RING - k) % RING, (z + k) % RING
        for half in range(2):
            if k < 4 or half == 0:
                here = block(above, core, half)
                copies.arrived(here, ups, (k - 1, half), up)
                spread(here, above, k, half, k < 3 or (k == 3 and half == 0), False, k)
            if k < 4 or half == 1:
                here = block(below, core, half)
                copies.arrived(here, downs, (k - 1, half), down)
                spread(
                    here,
                    below,
                    k,
                    half,
                    False,
                    k < 3 or (k == 3 and half == 1),
                    4 if k == 4 else 4 + k,
                )
        between(k)
    for slot in range(RING):
        g = (z + RING - slot) % RING if slot <= 4 else (z + slot - 4) % RING
        for half in range(2):
            copies.arrived(block(g, 1 - core, half), shares, (slot, half), partner)


def experts_kernel(
    ids_ref,
    weight_ref,
    in_ref,
    cot_ref,
    wg_ref,
    wu_ref,
    wd_ref,
    gg_ref,
    ug_ref,
    dg_ref,
    m_ref,
    src0,
    src1,
    x_far,
    x_near,
    r,
    wgu,
    wd,
    gu,
    hid,
    hid_t,
    p,
    pair_buf,
    out_up,
    in_up,
    out_down,
    in_down,
    sums,
    slots,
    chosen,
    mixed,
    *sems,
):
    (load_sem, *pairs) = sems
    (far_s, near_s, nshare_s, up_s, down_s, share_s, pair_s) = [
        (pairs[2 * i], pairs[2 * i + 1]) for i in range(7)
    ]
    (rup_s, rdown_s, back_s, gup_s, gdown_s, gshare_s) = [
        (pairs[2 * i], pairs[2 * i + 1]) for i in range(7, 13)
    ]
    sp, tp = lax.axis_index("sp"), lax.axis_index("tp")
    y, x = sp // SIDE, sp % SIDE
    z, core = tp // 2, tp % 2
    partner = (sp, z * 2 + 1 - core)
    up = (sp, ((z + 1) % RING) * 2 + core)
    down = (sp, ((z + RING - 1) % RING) * 2 + core)
    others = [partner, up, down]
    others += [(sp_at(dy, dx), tp) for dy, dx in OFFSETS if (dy, dx) != (0, 0)]
    barrier = pltpu.get_barrier_semaphore()
    for device in others:
        pl.semaphore_signal(barrier, inc=1, device_id=device, device_id_type=MESH)
    copies = Copies()
    tokens = in_ref.shape[0]

    loads = [
        pltpu.make_async_copy(wg_ref, wgu.at[:, pl.ds(0, HIDDEN)], load_sem.at[0]),
        pltpu.make_async_copy(wu_ref, wgu.at[:, pl.ds(HIDDEN, HIDDEN)], load_sem.at[1]),
        pltpu.make_async_copy(wd_ref, wd, load_sem.at[2]),
    ]
    for load in loads:
        load.start()

    n_experts = N_OFF
    expert = lax.broadcasted_iota(jnp.int32, (n_experts, tokens), 0)
    one = [(ids_ref[k : k + 1, :] == expert).astype(F32) for k in range(2)]
    earlier = (
        lax.broadcasted_iota(jnp.int32, (tokens, tokens), 0)
        < lax.broadcasted_iota(jnp.int32, (tokens, tokens), 1)
    ).astype(BF16)
    before = jnp.dot((one[0] + one[1]).astype(BF16), earlier, preferred_element_type=F32)
    place = jnp.zeros((n_experts, tokens), jnp.int32)
    for o, (dy, dx) in enumerate(OFFSETS):
        place = jnp.where(
            expert == ((y + dy) % SIDE) * SIDE + (x + dx) % SIDE, o * CAP, place
        )
    row_of = before + place.astype(F32)
    row_f = [jnp.sum(one[k] * row_of, axis=0, keepdims=True) for k in range(2)]
    row = [value.astype(jnp.int32) for value in row_f]

    def column(value):
        return jnp.transpose(jnp.broadcast_to(value, (128, tokens)))

    for k, src in enumerate((src0, src1)):
        scale = column(weight_ref[k : k + 1, :])
        for j in range(D // 128):
            part = pl.ds(j * 128, 128)
            scaled = (scale * cot_ref[:, part].astype(F32)).astype(BF16)
            src[:, part] = jnp.where(core == 0, in_ref[:, part], scaled)

    def picked(at):
        return (
            jnp.dot((row[0] == at).astype(BF16), src0[...], preferred_element_type=F32)
            + jnp.dot((row[1] == at).astype(BF16), src1[...], preferred_element_type=F32)
        ).astype(BF16)

    def fill(first, count):
        at = lax.broadcasted_iota(jnp.int32, (count * CAP, tokens), 0) + first * CAP
        x_near[pl.ds(first, count)] = picked(at).reshape(count, RING, 8, D)

    def send_near(first, count):
        for o in range(first, first + count):
            if o == LOCAL:
                copies.send(x_near.at[o], r.at[core, o], nshare_s, o, partner)
            else:
                copies.send(
                    x_near.at[o], r.at[core, o], near_s, o, (sp_at(*OFFSETS[o]), tp)
                )

    index = lax.broadcasted_iota(jnp.int32, (len(FAR) * 8, tokens), 0)
    x_far[...] = picked((FAR_AT + index // 8) * CAP + z * 8 + index % 8).reshape(len(FAR), 8, D)
    fill(0, 4)
    pl.semaphore_wait(barrier, len(others))
    for i, offset in enumerate(FAR):
        copies.send(
            x_far.at[i], r.at[core, FAR_AT + i, z], far_s, i, (sp_at(*offset), tp)
        )
    fill(4, 4)
    send_near(0, 4)
    fill(8, 3)
    send_near(4, 4)
    send_near(8, 3)
    r[core, LOCAL] = x_near[LOCAL]

    def far(g, c, half):
        start, size = HALVES[half]
        return r.at[c, pl.ds(FAR_AT + start, size), g]

    def forward(first, count):
        for o in range(first, first + count):
            if o != LOCAL:
                copies.arrived(r.at[core, o], near_s, o, partner)
                copies.send(r.at[core, o], r.at[core, o], nshare_s, o, partner)

    def shared(first, count):
        for o in range(first, first + count):
            copies.arrived(r.at[1 - core, o], nshare_s, o, partner)

    def forward_group(first, count):
        span = pl.ds(first * CAP, count * CAP)
        rows_in = r[0, pl.ds(first, count)].reshape(count * CAP, D)
        rows_cot = r[1, pl.ds(first, count)].reshape(count * CAP, D)
        both = jnp.dot(rows_in, wgu[...], preferred_element_type=F32)
        gate_pre, up_pre = both[:, :HIDDEN], both[:, HIDDEN:]
        hidden_cot = contract(rows_cot, wd[...], 1, 1)
        sigma = jax.nn.sigmoid(gate_pre)
        hid[span, :] = (gate_pre * sigma * up_pre).astype(BF16)
        gu[span, pl.ds(0, HIDDEN)] = (
            hidden_cot * up_pre * sigma * (1.0 + gate_pre * (1.0 - sigma))
        ).astype(BF16)
        gu[span, pl.ds(HIDDEN, HIDDEN)] = (hidden_cot * gate_pre * sigma).astype(BF16)

    def between(k):
        if k == 0:
            forward(0, 4)
            for load in loads:
                load.wait()
            shared(0, 4)
            forward_group(0, 4)
        if k == 2:
            forward(4, 5)
        if k == 3:
            shared(4, 5)
            forward_group(4, 5)
        if k == 4:
            forward(9, 2)
            shared(9, 2)
            forward_group(9, 2)

    for i in range(len(FAR)):
        copies.arrived(r.at[core, FAR_AT + i, z], far_s, i, partner)
    spread_ring(
        copies,
        far,
        lambda half: far(z, core, half),
        core,
        z,
        up,
        down,
        partner,
        up_s,
        down_s,
        share_s,
        between,
    )
    forward_group(FAR_AT, len(FAR))

    half_rows = ROWS // 2

    def at_z(d):
        return (z + RING + d) % RING

    def chunk(d):
        g = at_z(d)
        total = contract(
            gu[...], wgu[pl.ds(pl.multiple_of(g * 256, 256), 256), :], 1, 1
        ).astype(BF16)
        p[0, g] = total[:, :128]
        p[1, g] = total[:, 128:]
        copies.send(p.at[1 - core, g], pair_buf.at[g], pair_s, d % RING, partner)

    def paired(d):
        copies.arrived(pair_buf.at[at_z(d)], pair_s, d % RING, partner)

    def span(half):
        return pl.ds(half * half_rows, half_rows)

    def own(d, half):
        g = at_z(d)
        return p[core, g, span(half), :].astype(F32) + pair_buf[g, span(half), :].astype(F32)

    def go(hop, half_up, half_down):
        copies.send(
            out_up.at[hop, span(half_up)], in_up.at[hop, span(half_up)], rup_s, (hop, half_up), up
        )
        copies.send(
            out_down.at[hop, span(half_down)],
            in_down.at[hop, span(half_down)],
            rdown_s,
            (hop, half_down),
            down,
        )

    def came(buf, sem, hop, half):
        copies.arrived(buf.at[hop, span(half)], sem, (hop, half), partner)
        return buf[hop, span(half), :].astype(F32)

    def weight_grads(i):
        part = pl.ds(i * 256, 256)
        rows_in = r[0, :, :, :, part].reshape(ROWS, 256)
        rows_cot = r[1, :, :, :, part].reshape(ROWS, 256)
        both = contract(rows_in, gu[...], 0, 0).astype(BF16)
        gg_ref[part, :] = both[:, :HIDDEN]
        ug_ref[part, :] = both[:, HIDDEN:]
        dg_ref[:, part] = jnp.dot(hid_t[...], rows_cot, preferred_element_type=F32).astype(BF16)

    chunk(4)
    chunk(3)
    paired(4)
    out_up[0, span(0), :] = own(4, 0).astype(BF16)
    out_down[0, span(1), :] = own(-4, 1).astype(BF16)
    go(0, 0, 1)
    chunk(-3)
    paired(3)
    paired(-3)
    out_up[1, span(1), :] = own(3, 1).astype(BF16)
    out_down[1, span(0), :] = own(-3, 0).astype(BF16)
    go(1, 1, 0)
    chunk(2)
    chunk(-2)
    for hop in range(1, 4):
        d = 4 - hop
        if hop > 1:
            paired(d)
            paired(-d)
        out_up[hop, span(0), :] = (came(in_up, rup_s, hop - 1, 0) + own(d, 0)).astype(BF16)
        out_down[hop, span(1), :] = (came(in_down, rdown_s, hop - 1, 1) + own(-d, 1)).astype(BF16)
        go(hop, 0, 1)
        if hop == 1:
            chunk(1)
            chunk(-1)
        if hop > 1:
            out_up[hop, span(1), :] = (came(in_up, rup_s, hop - 1, 1) + own(d, 1)).astype(BF16)
            out_down[hop, span(0), :] = (came(in_down, rdown_s, hop - 1, 0) + own(-d, 0)).astype(
                BF16
            )
            go(hop, 1, 0)
        if hop == 2:
            chunk(0)
            hid_t[...] = jnp.transpose(hid[...])
            weight_grads(0)
        if hop == 3:
            weight_grads(1)
            weight_grads(2)
    paired(0)
    for half in range(2):
        sums[span(half), :] = (
            own(0, half) + came(in_up, rup_s, 3, half) + came(in_down, rdown_s, 3, half)
        ).astype(BF16)
    for o in reversed(range(N_OFF)):
        if o != LOCAL:
            dy, dx = OFFSETS[o]
            part = pl.ds(o * CAP, CAP)
            copies.send(sums.at[part], slots.at[part], back_s, o, (sp_at(-dy, -dx), tp))
    here = pl.ds(LOCAL * CAP, CAP)
    slots[here, :] = sums[here, :]
    where = [column(value).astype(jnp.int32) for value in row_f]
    for j in range(ROWS // 128):
        at = lax.broadcasted_iota(jnp.int32, (tokens, 128), 1) + j * 128
        chosen[:, pl.ds(j * 128, 128)] = ((where[0] == at) | (where[1] == at)).astype(BF16)
    weight_grads(3)
    weight_grads(4)
    for o in range(N_OFF):
        if o != LOCAL:
            copies.arrived(slots.at[pl.ds(o * CAP, CAP)], back_s, o, partner)
    total = jnp.dot(chosen[...], slots[...], preferred_element_type=F32)
    mine = pl.ds(pl.multiple_of(tp * 128, 128), 128)
    mixed[...] = (cot_ref[:, mine].astype(F32) + total).astype(BF16)

    half_tokens = tokens // 2

    def block(g, c, half):
        return m_ref.at[
            pl.ds(half * half_tokens, half_tokens),
            pl.ds(pl.multiple_of((g * 2 + c) * 128, 128), 128),
        ]

    def between_gather(k):
        if k == 0:
            m_ref[:, mine] = mixed[...]
            weight_grads(5)
        if k == 1:
            weight_grads(6)
        if k == 2:
            weight_grads(7)

    spread_ring(
        copies,
        block,
        lambda half: mixed.at[pl.ds(half * half_tokens, half_tokens)],
        core,
        z,
        up,
        down,
        partner,
        gup_s,
        gdown_s,
        gshare_s,
        between_gather,
    )
    copies.finish()


def experts(ids, weight, rows_in, cotangent, w_gate, w_up, w_down):
    dma = pltpu.SemaphoreType.DMA
    tokens = cotangent.shape[0]
    vmem = pl.BlockSpec(memory_space=pltpu.VMEM)
    anywhere = pl.BlockSpec(memory_space=pl.ANY)

    def both(*shape):
        return [dma(shape), dma(shape)]

    def buf(*shape):
        return pltpu.VMEM(shape, BF16)

    return pl.pallas_call(
        experts_kernel,
        out_shape=(
            jax.ShapeDtypeStruct((D, HIDDEN), BF16),
            jax.ShapeDtypeStruct((D, HIDDEN), BF16),
            jax.ShapeDtypeStruct((HIDDEN, D), BF16),
            jax.ShapeDtypeStruct((tokens, D), BF16),
        ),
        in_specs=[vmem] * 4 + [anywhere] * 3,
        out_specs=(vmem,) * 4,
        scratch_shapes=[
            buf(tokens, D),
            buf(tokens, D),
            buf(len(FAR), 8, D),
            buf(FAR_AT, RING, 8, D),
            buf(2, N_OFF, RING, 8, D),
            buf(D, 2 * HIDDEN),
            buf(HIDDEN, D),
            buf(ROWS, 2 * HIDDEN),
            buf(ROWS, HIDDEN),
            buf(HIDDEN, ROWS),
            buf(2, RING, ROWS, 128),
            buf(RING, ROWS, 128),
            buf(4, ROWS, 128),
            buf(4, ROWS, 128),
            buf(4, ROWS, 128),
            buf(4, ROWS, 128),
            buf(ROWS, 128),
            buf(ROWS, 128),
            buf(tokens, ROWS),
            buf(tokens, 128),
            dma((3,)),
            *both(len(FAR)),
            *both(FAR_AT),
            *both(FAR_AT),
            *both(4, 2),
            *both(4, 2),
            *both(RING, 2),
            *both(RING),
            *both(4, 2),
            *both(4, 2),
            *both(N_OFF),
            *both(4, 2),
            *both(4, 2),
            *both(RING, 2),
        ],
        compiler_params=pltpu.CompilerParams(
            collective_id=0, has_side_effects=True, vmem_limit_bytes=60 << 20
        ),
        name="experts",
    )(ids, weight, rows_in, cotangent, w_gate, w_up, w_down)


def cut_along(value, dim, devices):
    before, after = (value.shape[:dim], value.shape[dim + 1 :])
    return jnp.moveaxis(value.reshape(*before, devices, -1, *after), dim, 0)


def sent_and_summed(value, axis, dim):
    devices = lax.axis_size(axis)
    tiles = lax.all_to_all(cut_along(value, dim, devices), axis, 0, 0, tiled=True)
    return jnp.sum(tiles.astype(F32), axis=0)


def of_everyone(value, axis):
    copies = jnp.broadcast_to(value, (lax.axis_size(axis), *value.shape))
    everything = lax.all_to_all(copies, axis, split_axis=0, concat_axis=0, tiled=True)
    return jnp.sum(everything, axis=0)


def from_behind(value, axis, by):
    devices = lax.axis_size(axis)
    pairs = [(i, i + by) for i in range(devices) if 0 <= i + by < devices]
    return lax.ppermute(value, axis, pairs)


def on_device(
    saved_input,
    cotangent,
    expert_ids,
    route_weight,
    w_gate,
    w_up,
    w_down,
    w_out,
    channel_gain,
    conv_taps,
    glu_value,
    glu_gate,
    conv_out,
    norm_mean,
    norm_rstd,
):
    tokens_here = cotangent.shape[0]
    gate_grad, up_grad, down_grad, mixed_cot = experts(
        expert_ids.T, route_weight.T, saved_input, cotangent, w_gate[0], w_up[0], w_down[0]
    )

    centered = (conv_out.astype(F32) - norm_mean[None, :]) * norm_rstd[None, :]
    normed = centered * channel_gain[:, None]
    sigma = jax.nn.sigmoid(normed)
    output_act = (normed * sigma).astype(BF16)
    proj_grad = sent_and_summed(contract(mixed_cot, output_act, 0, 1).astype(BF16), "sp", 0)
    act_cot = contract(w_out, mixed_cot, 0, 1)
    norm_cot = act_cot * sigma * (1.0 + normed * (1.0 - sigma)) * channel_gain[:, None]
    sums = of_everyone(
        jnp.stack([jnp.sum(norm_cot, axis=0), jnp.sum(norm_cot * centered, axis=0)]), "tp"
    )
    first_sum, second_sum = sums[0], sums[1]
    conv_cot = norm_rstd[None, :] * (
        norm_cot - first_sum[None, :] / C - centered * second_sum[None, :] / C
    )
    reach = conv_taps.shape[0] - 1
    rim = from_behind(conv_cot[:, :reach], "sp", -1)
    padded = jnp.concatenate([conv_cot, rim], axis=1)
    glu_cot = conv_taps[0][:, None] * padded[:, :tokens_here]
    for lag in range(1, reach + 1):
        glu_cot = glu_cot + conv_taps[lag][:, None] * padded[:, lag : lag + tokens_here]
    gate_sigma = jax.nn.sigmoid(glu_gate.astype(F32))
    value_grad = (glu_cot * gate_sigma).astype(BF16)
    gate_in_grad = (glu_cot * glu_value.astype(F32) * gate_sigma * (1.0 - gate_sigma)).astype(BF16)
    return (gate_grad[None], up_grad[None], down_grad[None], proj_grad, value_grad, gate_in_grad)


def solution(mesh):
    in_specs = (
        P("sp", None),
        P("sp", None),
        P("sp", None),
        P("sp", None),
        P("sp", None, "tp"),
        P("sp", None, "tp"),
        P("sp", "tp", None),
        P(None, "tp"),
        P("tp"),
        P(None, "tp"),
        P("tp", "sp"),
        P("tp", "sp"),
        P("tp", "sp"),
        P("sp"),
        P("sp"),
    )
    out_specs = (
        P("sp", None, "tp"),
        P("sp", None, "tp"),
        P("sp", "tp", None),
        P("sp", "tp"),
        P("tp", "sp"),
        P("tp", "sp"),
    )
    return jax.shard_map(
        on_device, mesh=mesh, in_specs=in_specs, out_specs=out_specs, check_vma=False
    )
```

```python
import jax
import jax.numpy as jnp
from jax import lax
from jax.experimental import pallas as pl
from jax.experimental.pallas import tpu as pltpu
from jax.sharding import PartitionSpec as P

D = 2048
C = 2048
HIDDEN = 384
SIDE = 4
RING = 8
CAP = 64
BF16 = jnp.bfloat16
F32 = jnp.float32
MESH = pl.DeviceIdType.MESH

NEXT = ((0, 1), (0, 3), (1, 0), (3, 0))
CORNER = ((1, 1), (3, 3), (1, 3), (3, 1))
HERE = ((0, 0),)
ACROSS = ((0, 2), (2, 0))
FAR = ((1, 2), (3, 2), (2, 1), (2, 3), (2, 2))
OFFSETS = NEXT + CORNER + HERE + ACROSS + FAR
N_OFF = len(OFFSETS)
LOCAL = OFFSETS.index((0, 0))
FAR_AT = N_OFF - len(FAR)
HALVES = ((0, 3), (3, 2))
ROWS = N_OFF * CAP
EARLY = LOCAL + 1
SPANS = ((0, EARLY * CAP), (EARLY * CAP, ROWS - EARLY * CAP))


def sp_at(dy, dx):
    sp = lax.axis_index("sp")
    y, x = sp // SIDE, sp % SIDE
    return ((y + dy) % SIDE) * SIDE + (x + dx) % SIDE


def contract(left, right, left_dim, right_dim):
    return lax.dot_general(
        left, right, (((left_dim,), (right_dim,)), ((), ())), preferred_element_type=F32
    )


class Copies:
    def __init__(self):
        self.started = []

    def send(self, src, dst, sems, at, device):
        copy = pltpu.make_async_remote_copy(
            src_ref=src,
            dst_ref=dst,
            send_sem=sems[0].at[at],
            recv_sem=sems[1].at[at],
            device_id=device,
            device_id_type=MESH,
        )
        copy.start()
        self.started.append(copy)

    def arrived(self, dst, sems, at, device):
        pltpu.make_async_remote_copy(
            src_ref=dst,
            dst_ref=dst,
            send_sem=sems[0].at[at],
            recv_sem=sems[1].at[at],
            device_id=device,
            device_id_type=MESH,
        ).wait_recv()

    def finish(self):
        for copy in self.started:
            copy.wait_send()


def spread_ring(copies, block, source, core, z, up, down, partner, ups, downs, shares, between):
    def spread(src, g, k, half, going_up, going_down, slot):
        dst = block(g, core, half)
        if going_up:
            copies.send(src, dst, ups, (k, half), up)
        if going_down:
            copies.send(src, dst, downs, (k, half), down)
        copies.send(src, dst, shares, (slot, half), partner)

    for half in range(2):
        spread(source(half), z, 0, half, True, True, 0)
    between(0)
    for k in range(1, 5):
        above, below = (z + RING - k) % RING, (z + k) % RING
        for half in range(2):
            if k < 4 or half == 0:
                here = block(above, core, half)
                copies.arrived(here, ups, (k - 1, half), up)
                spread(here, above, k, half, k < 3 or (k == 3 and half == 0), False, k)
            if k < 4 or half == 1:
                here = block(below, core, half)
                copies.arrived(here, downs, (k - 1, half), down)
                spread(
                    here,
                    below,
                    k,
                    half,
                    False,
                    k < 3 or (k == 3 and half == 1),
                    4 if k == 4 else 4 + k,
                )
        between(k)
    for slot in range(RING):
        g = (z + RING - slot) % RING if slot <= 4 else (z + slot - 4) % RING
        for half in range(2):
            copies.arrived(block(g, 1 - core, half), shares, (slot, half), partner)


def experts_kernel(
    ids_ref,
    weight_ref,
    in_ref,
    cot_ref,
    wg_ref,
    wu_ref,
    wd_ref,
    wo_ref,
    gain_ref,
    conv_ref,
    mean_ref,
    rstd_ref,
    gg_out,
    ug_out,
    dg_out,
    cc_ref,
    proj_ref,
    gg_ref,
    ug_ref,
    dg_ref,
    m_ref,
    src0,
    src1,
    x_far,
    x_near,
    r,
    wgu,
    wd,
    gu,
    hid,
    hid_t,
    p,
    pair_buf,
    out_up,
    in_up,
    out_down,
    in_down,
    sums,
    slots,
    chosen,
    mixed,
    act,
    factor,
    centered,
    total_out,
    total_in,
    proj_out,
    proj_in,
    rim,
    *sems,
):
    (load_sem, grad_sem, *pairs) = sems
    grads = []
    (far_s, near_s, nshare_s, up_s, down_s, share_s, pair_s) = [
        (pairs[2 * i], pairs[2 * i + 1]) for i in range(7)
    ]
    (rup_s, rdown_s, back_s, gup_s, gdown_s, gshare_s, total_s, proj_s, rim_s) = [
        (pairs[2 * i], pairs[2 * i + 1]) for i in range(7, 16)
    ]
    sp, tp = lax.axis_index("sp"), lax.axis_index("tp")
    y, x = sp // SIDE, sp % SIDE
    z, core = tp // 2, tp % 2
    partner = (sp, z * 2 + 1 - core)
    up = (sp, ((z + 1) % RING) * 2 + core)
    down = (sp, ((z + RING - 1) % RING) * 2 + core)
    n_tp = 2 * RING
    others = [(sp, (tp + d) % n_tp) for d in range(1, n_tp)]
    others += [(sp_at(dy, dx), tp) for dy, dx in OFFSETS if (dy, dx) != (0, 0)]
    barrier = pltpu.get_barrier_semaphore()
    for device in others:
        pl.semaphore_signal(barrier, inc=1, device_id=device, device_id_type=MESH)
    copies = Copies()
    tokens = in_ref.shape[0]

    loads = [
        pltpu.make_async_copy(wg_ref, wgu.at[:, pl.ds(0, HIDDEN)], load_sem.at[0]),
        pltpu.make_async_copy(wu_ref, wgu.at[:, pl.ds(HIDDEN, HIDDEN)], load_sem.at[1]),
        pltpu.make_async_copy(wd_ref, wd, load_sem.at[2]),
    ]
    for load in loads:
        load.start()

    n_experts = N_OFF
    expert = lax.broadcasted_iota(jnp.int32, (n_experts, tokens), 0)
    one = [(ids_ref[k : k + 1, :] == expert).astype(F32) for k in range(2)]
    earlier = (
        lax.broadcasted_iota(jnp.int32, (tokens, tokens), 0)
        < lax.broadcasted_iota(jnp.int32, (tokens, tokens), 1)
    ).astype(BF16)
    before = jnp.dot((one[0] + one[1]).astype(BF16), earlier, preferred_element_type=F32)
    place = jnp.zeros((n_experts, tokens), jnp.int32)
    for o, (dy, dx) in enumerate(OFFSETS):
        place = jnp.where(
            expert == ((y + dy) % SIDE) * SIDE + (x + dx) % SIDE, o * CAP, place
        )
    row_of = before + place.astype(F32)
    row_f = [jnp.sum(one[k] * row_of, axis=0, keepdims=True) for k in range(2)]
    row = [value.astype(jnp.int32) for value in row_f]

    def column(value):
        return jnp.transpose(jnp.broadcast_to(value, (128, tokens)))

    for k, src in enumerate((src0, src1)):
        scale = column(weight_ref[k : k + 1, :])
        for j in range(D // 128):
            part = pl.ds(j * 128, 128)
            scaled = (scale * cot_ref[:, part].astype(F32)).astype(BF16)
            src[:, part] = jnp.where(core == 0, in_ref[:, part], scaled)

    def picked(at):
        return (
            jnp.dot((row[0] == at).astype(BF16), src0[...], preferred_element_type=F32)
            + jnp.dot((row[1] == at).astype(BF16), src1[...], preferred_element_type=F32)
        ).astype(BF16)

    def fill(first, count):
        at = lax.broadcasted_iota(jnp.int32, (count * CAP, tokens), 0) + first * CAP
        x_near[pl.ds(first, count)] = picked(at).reshape(count, RING, 8, D)

    def send_near(first, count):
        for o in range(first, first + count):
            if o == LOCAL:
                copies.send(x_near.at[o], r.at[core, o], nshare_s, o, partner)
            else:
                copies.send(
                    x_near.at[o], r.at[core, o], near_s, o, (sp_at(*OFFSETS[o]), tp)
                )

    index = lax.broadcasted_iota(jnp.int32, (len(FAR) * 8, tokens), 0)
    x_far[...] = picked((FAR_AT + index // 8) * CAP + z * 8 + index % 8).reshape(len(FAR), 8, D)
    fill(0, 4)
    pl.semaphore_wait(barrier, len(others))
    for i, offset in enumerate(FAR):
        copies.send(
            x_far.at[i], r.at[core, FAR_AT + i, z], far_s, i, (sp_at(*offset), tp)
        )
    fill(4, 4)
    send_near(0, 4)
    fill(8, 3)
    send_near(4, 4)
    send_near(8, 3)
    r[core, LOCAL] = x_near[LOCAL]

    def prepare():
        gain = gain_ref[...]
        rstd = column(rstd_ref[...])
        cent = (jnp.transpose(conv_ref[...].astype(F32)) - column(mean_ref[...])) * rstd
        normed = cent * gain
        sigma = jax.nn.sigmoid(normed)
        centered[...] = cent
        factor[...] = sigma * (1.0 + normed * (1.0 - sigma)) * gain
        act[...] = jnp.transpose(normed * sigma).astype(BF16)
        where = [column(value).astype(jnp.int32) for value in row_f]
        for j in range(ROWS // 128):
            at = lax.broadcasted_iota(jnp.int32, (tokens, 128), 1) + j * 128
            chosen[:, pl.ds(j * 128, 128)] = ((where[0] == at) | (where[1] == at)).astype(BF16)

    def far(g, c, half):
        start, size = HALVES[half]
        return r.at[c, pl.ds(FAR_AT + start, size), g]

    def forward(first, count):
        for o in range(first, first + count):
            if o != LOCAL:
                copies.arrived(r.at[core, o], near_s, o, partner)
                copies.send(r.at[core, o], r.at[core, o], nshare_s, o, partner)

    def shared(first, count):
        for o in range(first, first + count):
            copies.arrived(r.at[1 - core, o], nshare_s, o, partner)

    def forward_group(first, count):
        span = pl.ds(first * CAP, count * CAP)
        rows_in = r[0, pl.ds(first, count)].reshape(count * CAP, D)
        rows_cot = r[1, pl.ds(first, count)].reshape(count * CAP, D)
        both = jnp.dot(rows_in, wgu[...], preferred_element_type=F32)
        gate_pre, up_pre = both[:, :HIDDEN], both[:, HIDDEN:]
        hidden_cot = contract(rows_cot, wd[...], 1, 1)
        sigma = jax.nn.sigmoid(gate_pre)
        hid[span, :] = (gate_pre * sigma * up_pre).astype(BF16)
        gu[span, pl.ds(0, HIDDEN)] = (
            hidden_cot * up_pre * sigma * (1.0 + gate_pre * (1.0 - sigma))
        ).astype(BF16)
        gu[span, pl.ds(HIDDEN, HIDDEN)] = (hidden_cot * gate_pre * sigma).astype(BF16)

    def at_z(d):
        return (z + RING + d) % RING

    def span(half):
        return pl.ds(*SPANS[half])

    def chunk(d, half):
        g = at_z(d)
        total = contract(
            gu[span(half), :], wgu[pl.ds(pl.multiple_of(g * 256, 256), 256), :], 1, 1
        ).astype(BF16)
        p[0, g, span(half), :] = total[:, :128]
        p[1, g, span(half), :] = total[:, 128:]
        copies.send(
            p.at[1 - core, g, span(half)],
            pair_buf.at[g, span(half)],
            pair_s,
            (d % RING, half),
            partner,
        )

    def own(d, half):
        g = at_z(d)
        copies.arrived(pair_buf.at[g, span(half)], pair_s, (d % RING, half), partner)
        return p[core, g, span(half), :].astype(F32) + pair_buf[g, span(half), :].astype(F32)

    def came(buf, sem, hop, half):
        copies.arrived(buf.at[hop, span(half)], sem, (hop, half), partner)
        return buf[hop, span(half), :].astype(F32)

    def step_up(hop, half):
        total = own(4 - hop, half)
        if hop > half:
            total = total + came(in_up, rup_s, hop - 1, half)
        out_up[hop, span(half), :] = total.astype(BF16)

    def step_down(hop, half):
        total = own(hop - 4, half)
        if hop > 1 - half:
            total = total + came(in_down, rdown_s, hop - 1, half)
        out_down[hop, span(half), :] = total.astype(BF16)

    def go_up(hop, half):
        here = (hop, span(half))
        copies.send(out_up.at[here], in_up.at[here], rup_s, (hop, half), up)

    def go_down(hop, half):
        here = (hop, span(half))
        copies.send(out_down.at[here], in_down.at[here], rdown_s, (hop, half), down)

    def weight_grads(i):
        part = pl.ds(i * 256, 256)
        rows_in = r[0, :, :, :, part].reshape(ROWS, 256)
        rows_cot = r[1, :, :, :, part].reshape(ROWS, 256)
        both = contract(rows_in, gu[...], 0, 0).astype(BF16)
        gg_ref[part, :] = both[:, :HIDDEN]
        ug_ref[part, :] = both[:, HIDDEN:]
        dg_ref[:, part] = jnp.dot(hid_t[...], rows_cot, preferred_element_type=F32).astype(BF16)
        for j, (buf, out, at) in enumerate(
            ((gg_ref, gg_out, part), (ug_ref, ug_out, part), (dg_ref, dg_out, (slice(None), part)))
        ):
            grads.append(pltpu.make_async_copy(buf.at[at], out.at[at], grad_sem.at[i, j]))
            grads[-1].start()

    def between(k):
        if k == 0:
            prepare()
            for load in loads:
                load.wait()
        if k == 1:
            forward(0, 4)
        if k == 2:
            shared(0, 4)
            forward_group(0, 4)
        if k == 3:
            forward(4, 5)
            shared(4, 5)
            forward_group(4, 5)
            chunk(4, 0)
            chunk(-3, 0)
            step_up(0, 0)
            go_up(0, 0)
            step_down(1, 0)
            go_down(1, 0)
        if k == 4:
            forward(9, 2)
            chunk(3, 0)
            chunk(-2, 0)
            step_up(1, 0)
            go_up(1, 0)
            step_down(2, 0)
            go_down(2, 0)
            chunk(2, 0)
            chunk(-1, 0)
            chunk(1, 0)
            shared(9, 2)
            forward_group(9, 2)

    for i in range(len(FAR)):
        copies.arrived(r.at[core, FAR_AT + i, z], far_s, i, partner)
    spread_ring(
        copies,
        far,
        lambda half: far(z, core, half),
        core,
        z,
        up,
        down,
        partner,
        up_s,
        down_s,
        share_s,
        between,
    )
    forward_group(FAR_AT, len(FAR))
    chunk(4, 1)
    chunk(3, 1)
    step_up(1, 1)
    step_down(0, 1)
    go_up(1, 1)
    go_down(0, 1)
    step_up(2, 0)
    go_up(2, 0)
    step_down(3, 0)
    go_down(3, 0)
    chunk(-3, 1)
    chunk(2, 1)
    step_down(1, 1)
    go_down(1, 1)
    step_up(2, 1)
    go_up(2, 1)
    step_up(3, 0)
    go_up(3, 0)
    chunk(-2, 1)
    chunk(1, 1)
    chunk(0, 0)
    chunk(-1, 1)
    chunk(0, 1)
    hid_t[...] = jnp.transpose(hid[...])
    step_down(2, 1)
    go_down(2, 1)
    step_up(3, 1)
    go_up(3, 1)
    weight_grads(0)
    weight_grads(1)
    step_down(3, 1)
    go_down(3, 1)
    weight_grads(2)
    for half in range(2):
        sums[span(half), :] = (
            own(0, half) + came(in_up, rup_s, 3, half) + came(in_down, rdown_s, 3, half)
        ).astype(BF16)
    for o in reversed(range(N_OFF)):
        if o != LOCAL:
            dy, dx = OFFSETS[o]
            part = pl.ds(o * CAP, CAP)
            copies.send(sums.at[part], slots.at[part], back_s, o, (sp_at(-dy, -dx), tp))
    here = pl.ds(LOCAL * CAP, CAP)
    slots[here, :] = sums[here, :]
    weight_grads(3)
    weight_grads(4)
    for o in range(N_OFF):
        if o != LOCAL:
            copies.arrived(slots.at[pl.ds(o * CAP, CAP)], back_s, o, partner)
    total = jnp.dot(chosen[...], slots[...], preferred_element_type=F32)
    mine = pl.ds(pl.multiple_of(tp * 128, 128), 128)
    mixed[...] = (cot_ref[:, mine].astype(F32) + total).astype(BF16)

    half_tokens = tokens // 2

    def block(g, c, half):
        return m_ref.at[
            pl.ds(half * half_tokens, half_tokens),
            pl.ds(pl.multiple_of((g * 2 + c) * 128, 128), 128),
        ]

    def between_gather(k):
        if k == 0:
            m_ref[:, mine] = mixed[...]
            weight_grads(5)
        if k == 1:
            weight_grads(6)
        if k == 2:
            weight_grads(7)

    spread_ring(
        copies,
        block,
        lambda half: mixed.at[pl.ds(half * half_tokens, half_tokens)],
        core,
        z,
        up,
        down,
        partner,
        gup_s,
        gdown_s,
        gshare_s,
        between_gather,
    )

    act_cot = jnp.dot(m_ref[...], wo_ref[...], preferred_element_type=F32)
    norm_cot = act_cot * factor[...]
    for i, value in enumerate((norm_cot, norm_cot * centered[...])):
        whole = jnp.broadcast_to(jnp.sum(value, axis=1, keepdims=True), (tokens, 128))
        total_out[i : i + 1, :] = jnp.transpose(whole)[0:1, :]
    total_in[tp] = total_out[...]
    for d in range(1, n_tp):
        copies.send(total_out, total_in.at[tp], total_s, d, (sp, (tp + d) % n_tp))
    for s in range(N_OFF // 4):
        part = jnp.dot(act[...], m_ref[:, pl.ds(s * 512, 512)], preferred_element_type=F32)
        for i in range(4):
            proj_out[4 * s + i] = part[:, i * 128 : i * 128 + 128].astype(BF16)
    for o in range(N_OFF):
        if o != LOCAL:
            peer = sp_at(*OFFSETS[o])
            copies.send(proj_out.at[peer], proj_in.at[o], proj_s, o, (peer, tp))
    proj_in[LOCAL] = proj_out[sp]
    for d in range(1, n_tp):
        copies.arrived(total_in.at[(tp + n_tp - d) % n_tp], total_s, d, partner)
    totals = jnp.sum(total_in[...], axis=0)
    conv_cot = column(rstd_ref[...]) * (
        norm_cot - column(totals[0:1, :]) / C - centered[...] * (column(totals[1:2, :]) / C)
    )
    cc_ref[pl.ds(0, tokens), :] = conv_cot
    n_rim = rim.shape[1]
    rim[0] = conv_cot[:n_rim, :]
    copies.send(rim.at[0], rim.at[1], rim_s, 0, ((sp + N_OFF - 1) % N_OFF, tp))
    for o in range(N_OFF):
        if o != LOCAL:
            copies.arrived(proj_in.at[o], proj_s, o, partner)
    proj_ref[...] = jnp.sum(proj_in[...].astype(F32), axis=0)
    copies.arrived(rim.at[1], rim_s, 0, partner)
    cc_ref[pl.ds(tokens, n_rim), :] = jnp.where(sp == N_OFF - 1, 0.0, rim[1])
    for grad in grads:
        grad.wait()
    copies.finish()


def finish_kernel(
    gg_ref,
    ug_ref,
    dg_ref,
    cc_ref,
    proj_ref,
    taps_ref,
    value_ref,
    gate_ref,
    gg_out,
    ug_out,
    dg_out,
    proj_out,
    value_out,
    gate_out,
    gg,
    ug,
    dg,
    in_sem,
    out_sem,
):
    takes, gives = [], []
    for i, (src, buf, dst) in enumerate(
        ((gg_ref, gg, gg_out), (ug_ref, ug, ug_out), (dg_ref, dg, dg_out))
    ):
        size = src.shape[0] // 2
        for j in range(2):
            part = pl.ds(j * size, size)
            takes.append(pltpu.make_async_copy(src.at[part], buf.at[part], in_sem.at[i, j]))
            gives.append(pltpu.make_async_copy(buf.at[part], dst.at[part], out_sem.at[i, j]))
    for take in takes:
        take.start()
    tokens = value_ref.shape[1]
    total = taps_ref[0:1, :] * cc_ref[pl.ds(0, tokens), :]
    for lag in range(1, taps_ref.shape[0]):
        total = total + taps_ref[lag : lag + 1, :] * cc_ref[pl.ds(lag, tokens), :]
    for take, give in zip(takes, gives):
        take.wait()
        give.start()
    glu_cot = jnp.transpose(total)
    sigma = jax.nn.sigmoid(gate_ref[...].astype(F32))
    value_out[...] = (glu_cot * sigma).astype(BF16)
    gate_out[...] = (glu_cot * value_ref[...].astype(F32) * sigma * (1.0 - sigma)).astype(BF16)
    proj_out[...] = jnp.transpose(proj_ref[...])
    for give in gives:
        give.wait()


def finish(gg, ug, dg, cc, proj, taps, value, gate):
    vmem = pl.BlockSpec(memory_space=pltpu.VMEM)
    anywhere = pl.BlockSpec(memory_space=pl.ANY)

    def like(a):
        return jax.ShapeDtypeStruct(a.shape, a.dtype)

    return pl.pallas_call(
        finish_kernel,
        out_shape=(like(gg), like(ug), like(dg), like(proj), like(value), like(value)),
        in_specs=[anywhere] * 3 + [vmem] * 5,
        out_specs=(anywhere,) * 3 + (vmem,) * 3,
        scratch_shapes=[
            *[pltpu.VMEM(a.shape, a.dtype) for a in (gg, ug, dg)],
            pltpu.SemaphoreType.DMA((3, 2)),
            pltpu.SemaphoreType.DMA((3, 2)),
        ],
        compiler_params=pltpu.CompilerParams(vmem_limit_bytes=60 << 20),
        name="finish",
    )(gg, ug, dg, cc, proj, taps, value, gate)


def experts(
    ids, weight, rows_in, cotangent, w_gate, w_up, w_down, w_out, gain, conv_out, mean, rstd, reach
):
    dma = pltpu.SemaphoreType.DMA
    tokens = cotangent.shape[0]
    vmem = pl.BlockSpec(memory_space=pltpu.VMEM)
    anywhere = pl.BlockSpec(memory_space=pl.ANY)

    def both(*shape):
        return [dma(shape), dma(shape)]

    def buf(*shape):
        return pltpu.VMEM(shape, BF16)

    return pl.pallas_call(
        experts_kernel,
        out_shape=(
            jax.ShapeDtypeStruct((D, HIDDEN), BF16),
            jax.ShapeDtypeStruct((D, HIDDEN), BF16),
            jax.ShapeDtypeStruct((HIDDEN, D), BF16),
            jax.ShapeDtypeStruct((tokens + reach, 128), F32),
            jax.ShapeDtypeStruct((128, 128), F32),
        ),
        in_specs=[vmem] * 4 + [anywhere] * 3 + [vmem] * 5,
        out_specs=(anywhere,) * 3 + (vmem,) * 2,
        scratch_shapes=[
            buf(D, HIDDEN),
            buf(D, HIDDEN),
            buf(HIDDEN, D),
            buf(tokens, D),
            buf(tokens, D),
            buf(tokens, D),
            buf(len(FAR), 8, D),
            buf(FAR_AT, RING, 8, D),
            buf(2, N_OFF, RING, 8, D),
            buf(D, 2 * HIDDEN),
            buf(HIDDEN, D),
            buf(ROWS, 2 * HIDDEN),
            buf(ROWS, HIDDEN),
            buf(HIDDEN, ROWS),
            buf(2, RING, ROWS, 128),
            buf(RING, ROWS, 128),
            buf(4, ROWS, 128),
            buf(4, ROWS, 128),
            buf(4, ROWS, 128),
            buf(4, ROWS, 128),
            buf(ROWS, 128),
            buf(ROWS, 128),
            buf(tokens, ROWS),
            buf(tokens, 128),
            buf(128, tokens),
            pltpu.VMEM((tokens, 128), F32),
            pltpu.VMEM((tokens, 128), F32),
            pltpu.VMEM((2, tokens), F32),
            pltpu.VMEM((2 * RING, 2, tokens), F32),
            buf(N_OFF, 128, 128),
            buf(N_OFF, 128, 128),
            pltpu.VMEM((2, reach, 128), F32),
            dma((3,)),
            dma((RING, 3)),
            *both(len(FAR)),
            *both(FAR_AT),
            *both(FAR_AT),
            *both(4, 2),
            *both(4, 2),
            *both(RING, 2),
            *both(RING, 2),
            *both(4, 2),
            *both(4, 2),
            *both(N_OFF),
            *both(4, 2),
            *both(4, 2),
            *both(RING, 2),
            *both(2 * RING),
            *both(N_OFF),
            *both(1),
        ],
        compiler_params=pltpu.CompilerParams(
            collective_id=0, has_side_effects=True, vmem_limit_bytes=60 << 20
        ),
        name="experts",
    )(
        ids, weight, rows_in, cotangent, w_gate, w_up, w_down, w_out, gain, conv_out, mean, rstd
    )


def on_device(
    saved_input,
    cotangent,
    expert_ids,
    route_weight,
    w_gate,
    w_up,
    w_down,
    w_out,
    channel_gain,
    conv_taps,
    glu_value,
    glu_gate,
    conv_out,
    norm_mean,
    norm_rstd,
):
    reach = 32
    parts = experts(
        expert_ids.T,
        route_weight.T,
        saved_input,
        cotangent,
        w_gate[0],
        w_up[0],
        w_down[0],
        w_out,
        channel_gain[None],
        conv_out,
        norm_mean[None],
        norm_rstd[None],
        reach,
    )
    gate_grad, up_grad, down_grad, proj_grad, value_grad, gate_in_grad = finish(
        *parts, conv_taps, glu_value, glu_gate
    )
    return (
        gate_grad[None],
        up_grad[None],
        down_grad[None],
        proj_grad,
        value_grad,
        gate_in_grad,
    )


def solution(mesh):
    in_specs = (
        P("sp", None),
        P("sp", None),
        P("sp", None),
        P("sp", None),
        P("sp", None, "tp"),
        P("sp", None, "tp"),
        P("sp", "tp", None),
        P(None, "tp"),
        P("tp"),
        P(None, "tp"),
        P("tp", "sp"),
        P("tp", "sp"),
        P("tp", "sp"),
        P("sp"),
        P("sp"),
    )
    out_specs = (
        P("sp", None, "tp"),
        P("sp", None, "tp"),
        P("sp", "tp", None),
        P("sp", "tp"),
        P("tp", "sp"),
        P("tp", "sp"),
    )
    return jax.shard_map(
        on_device, mesh=mesh, in_specs=in_specs, out_specs=out_specs, check_vma=False
    )
```

```python
import jax
import jax.numpy as jnp
from jax import lax
from jax.experimental import pallas as pl
from jax.experimental.pallas import tpu as pltpu
from jax.sharding import PartitionSpec as P

D = 2048
C = 2048
HIDDEN = 384
SIDE = 4
RING = 8
CAP = 64
BF16 = jnp.bfloat16
F32 = jnp.float32
MESH = pl.DeviceIdType.MESH

NEXT = ((0, 1), (0, 3), (1, 0), (3, 0))
CORNER = ((1, 1), (3, 3), (1, 3), (3, 1))
HERE = ((0, 0),)
ACROSS = ((0, 2), (2, 0))
FAR = ((1, 2), (3, 2), (2, 1), (2, 3), (2, 2))
OFFSETS = NEXT + ACROSS + HERE + CORNER + FAR
N_OFF = len(OFFSETS)
LOCAL = OFFSETS.index((0, 0))
FAR_AT = N_OFF - len(FAR)
HALVES = ((0, 3), (3, 2))
ROWS = N_OFF * CAP
SPANS = ((0, 7 * CAP), (7 * CAP, 4 * CAP), (11 * CAP, 5 * CAP))


def sp_at(dy, dx):
    sp = lax.axis_index("sp")
    y, x = sp // SIDE, sp % SIDE
    return ((y + dy) % SIDE) * SIDE + (x + dx) % SIDE


def contract(left, right, left_dim, right_dim):
    return lax.dot_general(
        left, right, (((left_dim,), (right_dim,)), ((), ())), preferred_element_type=F32
    )


class Copies:
    def __init__(self):
        self.started = []

    def send(self, src, dst, sems, at, device):
        copy = pltpu.make_async_remote_copy(
            src_ref=src,
            dst_ref=dst,
            send_sem=sems[0].at[at],
            recv_sem=sems[1].at[at],
            device_id=device,
            device_id_type=MESH,
        )
        copy.start()
        self.started.append(copy)

    def arrived(self, dst, sems, at, device):
        pltpu.make_async_remote_copy(
            src_ref=dst,
            dst_ref=dst,
            send_sem=sems[0].at[at],
            recv_sem=sems[1].at[at],
            device_id=device,
            device_id_type=MESH,
        ).wait_recv()

    def finish(self):
        for copy in self.started:
            copy.wait_send()


def spread_ring(copies, block, source, core, z, up, down, partner, ups, downs, shares, between):
    def spread(src, g, k, half, going_up, going_down, slot):
        dst = block(g, core, half)
        if going_up:
            copies.send(src, dst, ups, (k, half), up)
        if going_down:
            copies.send(src, dst, downs, (k, half), down)
        copies.send(src, dst, shares, (slot, half), partner)

    for half in range(2):
        spread(source(half), z, 0, half, True, True, 0)
    between(0)
    for k in range(1, 5):
        above, below = (z + RING - k) % RING, (z + k) % RING
        for half in range(2):
            if k < 4 or half == 0:
                here = block(above, core, half)
                copies.arrived(here, ups, (k - 1, half), up)
                spread(here, above, k, half, k < 3 or (k == 3 and half == 0), False, k)
            if k < 4 or half == 1:
                here = block(below, core, half)
                copies.arrived(here, downs, (k - 1, half), down)
                spread(
                    here,
                    below,
                    k,
                    half,
                    False,
                    k < 3 or (k == 3 and half == 1),
                    4 if k == 4 else 4 + k,
                )
        between(k)
    for slot in range(RING):
        g = (z + RING - slot) % RING if slot <= 4 else (z + slot - 4) % RING
        for half in range(2):
            copies.arrived(block(g, 1 - core, half), shares, (slot, half), partner)


def experts_kernel(
    ids_in,
    weight_in,
    rows_in_ref,
    cot_in,
    wg_ref,
    wu_ref,
    wd_ref,
    wo_in,
    gain_in,
    conv_in,
    mean_in,
    rstd_in,
    gg_out,
    ug_out,
    dg_out,
    cc_ref,
    proj_ref,
    ids_ref,
    weight_ref,
    in_ref,
    cot_ref,
    wo_ref,
    gain_ref,
    conv_ref,
    mean_ref,
    rstd_ref,
    gg_ref,
    ug_ref,
    dg_ref,
    m_ref,
    src0,
    src1,
    x_far,
    x_near,
    r,
    wgu,
    wd,
    gu,
    hid,
    hid_t,
    p,
    pair_buf,
    out_up,
    in_up,
    out_down,
    in_down,
    sums,
    slots,
    chosen,
    mixed,
    act,
    factor,
    centered,
    total_out,
    total_in,
    proj_out,
    proj_in,
    rim,
    blocks,
    *sems,
):
    (load_sem, grad_sem, *pairs) = sems
    firsts = [
        pltpu.make_async_copy(src, dst, load_sem.at[3 + i])
        for i, (src, dst) in enumerate(
            (
                (ids_in, ids_ref),
                (weight_in, weight_ref),
                (cot_in, cot_ref),
                (rows_in_ref, in_ref),
                (conv_in, conv_ref),
                (mean_in, mean_ref),
                (rstd_in, rstd_ref),
                (gain_in, gain_ref),
                (wo_in, wo_ref),
            )
        )
    ]
    for first in firsts:
        first.start()
    grads = []
    (far_s, near_s, nshare_s, up_s, down_s, share_s, pair_s) = [
        (pairs[2 * i], pairs[2 * i + 1]) for i in range(7)
    ]
    (rup_s, rdown_s, back_s, gup_s, gdown_s, gshare_s, total_s, proj_s, rim_s) = [
        (pairs[2 * i], pairs[2 * i + 1]) for i in range(7, 16)
    ]
    sp, tp = lax.axis_index("sp"), lax.axis_index("tp")
    y, x = sp // SIDE, sp % SIDE
    z, core = tp // 2, tp % 2
    partner = (sp, z * 2 + 1 - core)
    up = (sp, ((z + 1) % RING) * 2 + core)
    down = (sp, ((z + RING - 1) % RING) * 2 + core)
    n_tp = 2 * RING
    others = [(sp, (tp + d) % n_tp) for d in range(1, n_tp)]
    others += [(sp_at(dy, dx), tp) for dy, dx in OFFSETS if (dy, dx) != (0, 0)]
    barrier = pltpu.get_barrier_semaphore()
    for device in others:
        pl.semaphore_signal(barrier, inc=1, device_id=device, device_id_type=MESH)
    copies = Copies()
    tokens = in_ref.shape[0]

    loads = [
        pltpu.make_async_copy(wg_ref, wgu.at[:, pl.ds(0, HIDDEN)], load_sem.at[0]),
        pltpu.make_async_copy(wu_ref, wgu.at[:, pl.ds(HIDDEN, HIDDEN)], load_sem.at[1]),
        pltpu.make_async_copy(wd_ref, wd, load_sem.at[2]),
    ]
    for load in loads:
        load.start()

    for first in firsts[:2]:
        first.wait()
    n_experts = N_OFF
    expert = lax.broadcasted_iota(jnp.int32, (n_experts, tokens), 0)
    one = [(ids_ref[k : k + 1, :] == expert).astype(F32) for k in range(2)]
    earlier = (
        lax.broadcasted_iota(jnp.int32, (tokens, tokens), 0)
        < lax.broadcasted_iota(jnp.int32, (tokens, tokens), 1)
    ).astype(BF16)
    before = jnp.dot((one[0] + one[1]).astype(BF16), earlier, preferred_element_type=F32)
    place = jnp.zeros((n_experts, tokens), jnp.int32)
    for o, (dy, dx) in enumerate(OFFSETS):
        place = jnp.where(
            expert == ((y + dy) % SIDE) * SIDE + (x + dx) % SIDE, o * CAP, place
        )
    row_of = before + place.astype(F32)
    row_f = [jnp.sum(one[k] * row_of, axis=0, keepdims=True) for k in range(2)]
    row = [value.astype(jnp.int32) for value in row_f]

    def column(value):
        return jnp.transpose(jnp.broadcast_to(value, (128, tokens)))

    for first in firsts[2:4]:
        first.wait()
    for k, src in enumerate((src0, src1)):
        scale = column(weight_ref[k : k + 1, :])
        for j in range(D // 128):
            part = pl.ds(j * 128, 128)
            scaled = (scale * cot_ref[:, part].astype(F32)).astype(BF16)
            src[:, part] = jnp.where(core == 0, in_ref[:, part], scaled)

    def picked(at):
        return (
            jnp.dot((row[0] == at).astype(BF16), src0[...], preferred_element_type=F32)
            + jnp.dot((row[1] == at).astype(BF16), src1[...], preferred_element_type=F32)
        ).astype(BF16)

    def fill(first, count):
        at = lax.broadcasted_iota(jnp.int32, (count * CAP, tokens), 0) + first * CAP
        x_near[pl.ds(first, count)] = picked(at).reshape(count, RING, 8, D)

    def send_near(first, count):
        for o in range(first, first + count):
            if o == LOCAL:
                copies.send(x_near.at[o], r.at[core, o], nshare_s, o, partner)
            else:
                copies.send(
                    x_near.at[o], r.at[core, o], near_s, o, (sp_at(*OFFSETS[o]), tp)
                )

    index = lax.broadcasted_iota(jnp.int32, (len(FAR) * 8, tokens), 0)
    x_far[...] = picked((FAR_AT + index // 8) * CAP + z * 8 + index % 8).reshape(len(FAR), 8, D)
    fill(0, 4)
    pl.semaphore_wait(barrier, len(others))
    for i, offset in enumerate(FAR):
        copies.send(
            x_far.at[i], r.at[core, FAR_AT + i, z], far_s, i, (sp_at(*offset), tp)
        )
    fill(4, 3)
    send_near(0, 4)
    fill(7, 4)
    send_near(4, 3)
    send_near(7, 4)
    r[core, LOCAL] = x_near[LOCAL]

    def prepare():
        for first in firsts[4:]:
            first.wait()
        gain = gain_ref[...]
        rstd = column(rstd_ref[...])
        cent = (jnp.transpose(conv_ref[...].astype(F32)) - column(mean_ref[...])) * rstd
        normed = cent * gain
        sigma = jax.nn.sigmoid(normed)
        centered[...] = cent
        factor[...] = sigma * (1.0 + normed * (1.0 - sigma)) * gain
        act[...] = jnp.transpose(normed * sigma).astype(BF16)
        where = [column(value).astype(jnp.int32) for value in row_f]
        for j in range(ROWS // 128):
            at = lax.broadcasted_iota(jnp.int32, (tokens, 128), 1) + j * 128
            chosen[:, pl.ds(j * 128, 128)] = ((where[0] == at) | (where[1] == at)).astype(BF16)

    def far(g, c, half):
        start, size = HALVES[half]
        return r.at[c, pl.ds(FAR_AT + start, size), g]

    def forward(first, count):
        for o in range(first, first + count):
            if o != LOCAL:
                copies.arrived(r.at[core, o], near_s, o, partner)
                copies.send(r.at[core, o], r.at[core, o], nshare_s, o, partner)

    def shared(first, count):
        for o in range(first, first + count):
            copies.arrived(r.at[1 - core, o], nshare_s, o, partner)

    def forward_group(first, count):
        span = pl.ds(first * CAP, count * CAP)
        rows_in = r[0, pl.ds(first, count)].reshape(count * CAP, D)
        rows_cot = r[1, pl.ds(first, count)].reshape(count * CAP, D)
        both = jnp.dot(rows_in, wgu[...], preferred_element_type=F32)
        gate_pre, up_pre = both[:, :HIDDEN], both[:, HIDDEN:]
        hidden_cot = contract(rows_cot, wd[...], 1, 1)
        sigma = jax.nn.sigmoid(gate_pre)
        hid[span, :] = (gate_pre * sigma * up_pre).astype(BF16)
        gu[span, pl.ds(0, HIDDEN)] = (
            hidden_cot * up_pre * sigma * (1.0 + gate_pre * (1.0 - sigma))
        ).astype(BF16)
        gu[span, pl.ds(HIDDEN, HIDDEN)] = (hidden_cot * gate_pre * sigma).astype(BF16)

    def at_z(d):
        return (z + RING + d) % RING

    def span(half):
        return pl.ds(*SPANS[half])

    def chunk(d, half):
        g = at_z(d)
        total = contract(
            gu[span(half), :], wgu[pl.ds(pl.multiple_of(g * 256, 256), 256), :], 1, 1
        ).astype(BF16)
        p[0, g, span(half), :] = total[:, :128]
        p[1, g, span(half), :] = total[:, 128:]
        copies.send(
            p.at[1 - core, g, span(half)],
            pair_buf.at[g, span(half)],
            pair_s,
            (d % RING, half),
            partner,
        )

    def own(d, half):
        g = at_z(d)
        copies.arrived(pair_buf.at[g, span(half)], pair_s, (d % RING, half), partner)
        return p[core, g, span(half), :].astype(F32) + pair_buf[g, span(half), :].astype(F32)

    def came(buf, sem, hop, half):
        copies.arrived(buf.at[hop, span(half)], sem, (hop, half), partner)
        return buf[hop, span(half), :].astype(F32)

    def step_up(hop, half):
        total = own(4 - hop, half)
        if hop > min(half, 1):
            total = total + came(in_up, rup_s, hop - 1, half)
        out_up[hop, span(half), :] = total.astype(BF16)

    def step_down(hop, half):
        total = own(hop - 4, half)
        if hop > 1 - min(half, 1):
            total = total + came(in_down, rdown_s, hop - 1, half)
        out_down[hop, span(half), :] = total.astype(BF16)

    def go_up(hop, half):
        here = (hop, span(half))
        copies.send(out_up.at[here], in_up.at[here], rup_s, (hop, half), up)

    def go_down(hop, half):
        here = (hop, span(half))
        copies.send(out_down.at[here], in_down.at[here], rdown_s, (hop, half), down)

    def weight_grads(i):
        part = pl.ds(i * 256, 256)
        rows_in = r[0, :, :, :, part].reshape(ROWS, 256)
        rows_cot = r[1, :, :, :, part].reshape(ROWS, 256)
        both = contract(rows_in, gu[...], 0, 0).astype(BF16)
        gg_ref[part, :] = both[:, :HIDDEN]
        ug_ref[part, :] = both[:, HIDDEN:]
        dg_ref[:, part] = jnp.dot(hid_t[...], rows_cot, preferred_element_type=F32).astype(BF16)
        for j, (buf, out, at) in enumerate(
            ((gg_ref, gg_out, part), (ug_ref, ug_out, part), (dg_ref, dg_out, (slice(None), part)))
        ):
            grads.append(pltpu.make_async_copy(buf.at[at], out.at[at], grad_sem.at[i, j]))
            grads[-1].start()

    def between(k):
        if k == 0:
            prepare()
            for load in loads:
                load.wait()
        if k == 1:
            forward(0, 4)
        if k == 2:
            shared(0, 4)
            forward_group(0, 4)
        if k == 3:
            forward(4, 3)
            shared(4, 3)
            forward_group(4, 3)
            chunk(4, 0)
            chunk(-3, 0)
            step_up(0, 0)
            go_up(0, 0)
            step_down(1, 0)
            go_down(1, 0)
        if k == 4:
            chunk(3, 0)
            chunk(-2, 0)
            step_up(1, 0)
            go_up(1, 0)
            step_down(2, 0)
            go_down(2, 0)
            chunk(2, 0)
            chunk(-1, 0)
            chunk(1, 0)
            forward(7, 4)
            shared(7, 4)
            forward_group(7, 4)
            chunk(4, 1)
            chunk(3, 1)
            step_down(0, 1)
            go_down(0, 1)
            step_up(1, 1)
            go_up(1, 1)

    def hop_on(ups, downs):
        for hop, half in ups:
            step_up(hop, half)
            go_up(hop, half)
        for hop, half in downs:
            step_down(hop, half)
            go_down(hop, half)

    for i in range(len(FAR)):
        copies.arrived(r.at[core, FAR_AT + i, z], far_s, i, partner)
    spread_ring(
        copies,
        far,
        lambda half: far(z, core, half),
        core,
        z,
        up,
        down,
        partner,
        up_s,
        down_s,
        share_s,
        between,
    )
    forward_group(FAR_AT, len(FAR))
    chunk(4, 2)
    chunk(3, 2)
    hop_on(((1, 2),), ((0, 2),))
    hop_on(((2, 0),), ((3, 0),))
    chunk(-3, 1)
    chunk(2, 1)
    hop_on(((2, 1),), ((1, 1),))
    chunk(-3, 2)
    chunk(2, 2)
    hop_on(((2, 2),), ((1, 2),))
    hop_on(((3, 0),), ())
    chunk(-2, 1)
    chunk(1, 1)
    hop_on(((3, 1),), ((2, 1),))
    chunk(-2, 2)
    chunk(1, 2)
    hop_on(((3, 2),), ((2, 2),))
    chunk(-1, 1)
    chunk(-1, 2)
    hid_t[...] = jnp.transpose(hid[...])
    weight_grads(0)
    hop_on((), ((3, 1),))
    hop_on((), ((3, 2),))
    for half in range(3):
        chunk(0, half)
    weight_grads(1)
    weight_grads(2)
    for half in range(3):
        sums[span(half), :] = (
            own(0, half) + came(in_up, rup_s, 3, half) + came(in_down, rdown_s, 3, half)
        ).astype(BF16)
    for o in reversed(range(N_OFF)):
        if o != LOCAL:
            dy, dx = OFFSETS[o]
            part = pl.ds(o * CAP, CAP)
            copies.send(sums.at[part], slots.at[part], back_s, o, (sp_at(-dy, -dx), tp))
    here = pl.ds(LOCAL * CAP, CAP)
    slots[here, :] = sums[here, :]
    weight_grads(3)
    weight_grads(4)
    for o in range(N_OFF):
        if o != LOCAL:
            copies.arrived(slots.at[pl.ds(o * CAP, CAP)], back_s, o, partner)
    total = jnp.dot(chosen[...], slots[...], preferred_element_type=F32)
    mine = pl.ds(pl.multiple_of(tp * 128, 128), 128)
    mixed[...] = (cot_ref[:, mine].astype(F32) + total).astype(BF16)

    half_tokens = tokens // 2

    def block(g, c, half):
        return blocks.at[g * 2 + c, pl.ds(half * half_tokens, half_tokens)]

    def between_gather(k):
        if k == 0:
            blocks[tp] = mixed[...]
            weight_grads(5)
        if k == 1:
            weight_grads(6)
        if k == 2:
            weight_grads(7)

    spread_ring(
        copies,
        block,
        lambda half: mixed.at[pl.ds(half * half_tokens, half_tokens)],
        core,
        z,
        up,
        down,
        partner,
        gup_s,
        gdown_s,
        gshare_s,
        between_gather,
    )

    for j in range(n_tp):
        m_ref[:, pl.ds(j * 128, 128)] = blocks[j]
    act_cot = jnp.dot(m_ref[...], wo_ref[...], preferred_element_type=F32)
    norm_cot = act_cot * factor[...]
    for i, value in enumerate((norm_cot, norm_cot * centered[...])):
        whole = jnp.broadcast_to(jnp.sum(value, axis=1, keepdims=True), (tokens, 128))
        total_out[i : i + 1, :] = jnp.transpose(whole)[0:1, :]
    total_in[tp] = total_out[...]
    for d in range(1, n_tp):
        copies.send(total_out, total_in.at[tp], total_s, d, (sp, (tp + d) % n_tp))
    for s in range(N_OFF // 4):
        part = jnp.dot(act[...], m_ref[:, pl.ds(s * 512, 512)], preferred_element_type=F32)
        for i in range(4):
            proj_out[4 * s + i] = part[:, i * 128 : i * 128 + 128].astype(BF16)
    for o in range(N_OFF):
        if o != LOCAL:
            peer = sp_at(*OFFSETS[o])
            copies.send(proj_out.at[peer], proj_in.at[o], proj_s, o, (peer, tp))
    proj_in[LOCAL] = proj_out[sp]
    for d in range(1, n_tp):
        copies.arrived(total_in.at[(tp + n_tp - d) % n_tp], total_s, d, partner)
    totals = jnp.sum(total_in[...], axis=0)
    conv_cot = column(rstd_ref[...]) * (
        norm_cot - column(totals[0:1, :]) / C - centered[...] * (column(totals[1:2, :]) / C)
    )
    cc_ref[pl.ds(0, tokens), :] = conv_cot
    n_rim = rim.shape[1]
    rim[0] = conv_cot[:n_rim, :]
    copies.send(rim.at[0], rim.at[1], rim_s, 0, ((sp + N_OFF - 1) % N_OFF, tp))
    for o in range(N_OFF):
        if o != LOCAL:
            copies.arrived(proj_in.at[o], proj_s, o, partner)
    proj_ref[...] = jnp.sum(proj_in[...].astype(F32), axis=0)
    copies.arrived(rim.at[1], rim_s, 0, partner)
    cc_ref[pl.ds(tokens, n_rim), :] = jnp.where(sp == N_OFF - 1, 0.0, rim[1])
    for grad in grads:
        grad.wait()
    copies.finish()


def finish_kernel(
    gg_ref,
    ug_ref,
    dg_ref,
    cc_ref,
    proj_ref,
    taps_ref,
    value_ref,
    gate_ref,
    gg_out,
    ug_out,
    dg_out,
    proj_out,
    value_out,
    gate_out,
    gg,
    ug,
    dg,
    in_sem,
    out_sem,
):
    takes, gives = [], []
    for i, (src, buf, dst) in enumerate(
        ((gg_ref, gg, gg_out), (ug_ref, ug, ug_out), (dg_ref, dg, dg_out))
    ):
        size = src.shape[0] // 2
        for j in range(2):
            part = pl.ds(j * size, size)
            takes.append(pltpu.make_async_copy(src.at[part], buf.at[part], in_sem.at[i, j]))
            gives.append(pltpu.make_async_copy(buf.at[part], dst.at[part], out_sem.at[i, j]))
    for take in takes:
        take.start()
    tokens = value_ref.shape[1]
    total = taps_ref[0:1, :] * cc_ref[pl.ds(0, tokens), :]
    for lag in range(1, taps_ref.shape[0]):
        total = total + taps_ref[lag : lag + 1, :] * cc_ref[pl.ds(lag, tokens), :]
    for take, give in zip(takes, gives):
        take.wait()
        give.start()
    glu_cot = jnp.transpose(total)
    sigma = jax.nn.sigmoid(gate_ref[...].astype(F32))
    value_out[...] = (glu_cot * sigma).astype(BF16)
    gate_out[...] = (glu_cot * value_ref[...].astype(F32) * sigma * (1.0 - sigma)).astype(BF16)
    proj_out[...] = jnp.transpose(proj_ref[...])
    for give in gives:
        give.wait()


def finish(gg, ug, dg, cc, proj, taps, value, gate):
    vmem = pl.BlockSpec(memory_space=pltpu.VMEM)
    anywhere = pl.BlockSpec(memory_space=pl.ANY)

    def like(a):
        return jax.ShapeDtypeStruct(a.shape, a.dtype)

    return pl.pallas_call(
        finish_kernel,
        out_shape=(like(gg), like(ug), like(dg), like(proj), like(value), like(value)),
        in_specs=[anywhere] * 3 + [vmem] * 5,
        out_specs=(anywhere,) * 3 + (vmem,) * 3,
        scratch_shapes=[
            *[pltpu.VMEM(a.shape, a.dtype) for a in (gg, ug, dg)],
            pltpu.SemaphoreType.DMA((3, 2)),
            pltpu.SemaphoreType.DMA((3, 2)),
        ],
        compiler_params=pltpu.CompilerParams(vmem_limit_bytes=60 << 20),
        name="finish",
    )(gg, ug, dg, cc, proj, taps, value, gate)


def experts(
    ids, weight, rows_in, cotangent, w_gate, w_up, w_down, w_out, gain, conv_out, mean, rstd, reach
):
    dma = pltpu.SemaphoreType.DMA
    tokens = cotangent.shape[0]
    vmem = pl.BlockSpec(memory_space=pltpu.VMEM)
    anywhere = pl.BlockSpec(memory_space=pl.ANY)

    def both(*shape):
        return [dma(shape), dma(shape)]

    def buf(*shape):
        return pltpu.VMEM(shape, BF16)

    return pl.pallas_call(
        experts_kernel,
        out_shape=(
            jax.ShapeDtypeStruct((D, HIDDEN), BF16),
            jax.ShapeDtypeStruct((D, HIDDEN), BF16),
            jax.ShapeDtypeStruct((HIDDEN, D), BF16),
            jax.ShapeDtypeStruct((tokens + reach, 128), F32),
            jax.ShapeDtypeStruct((128, 128), F32),
        ),
        in_specs=[anywhere] * 12,
        out_specs=(anywhere,) * 3 + (vmem,) * 2,
        scratch_shapes=[
            *[pltpu.VMEM(a.shape, a.dtype) for a in (ids, weight, rows_in, cotangent)],
            *[pltpu.VMEM(a.shape, a.dtype) for a in (w_out, gain, conv_out, mean, rstd)],
            buf(D, HIDDEN),
            buf(D, HIDDEN),
            buf(HIDDEN, D),
            buf(tokens, D),
            buf(tokens, D),
            buf(tokens, D),
            buf(len(FAR), 8, D),
            buf(FAR_AT, RING, 8, D),
            buf(2, N_OFF, RING, 8, D),
            buf(D, 2 * HIDDEN),
            buf(HIDDEN, D),
            buf(ROWS, 2 * HIDDEN),
            buf(ROWS, HIDDEN),
            buf(HIDDEN, ROWS),
            buf(2, RING, ROWS, 128),
            buf(RING, ROWS, 128),
            buf(4, ROWS, 128),
            buf(4, ROWS, 128),
            buf(4, ROWS, 128),
            buf(4, ROWS, 128),
            buf(ROWS, 128),
            buf(ROWS, 128),
            buf(tokens, ROWS),
            buf(tokens, 128),
            buf(128, tokens),
            pltpu.VMEM((tokens, 128), F32),
            pltpu.VMEM((tokens, 128), F32),
            pltpu.VMEM((2, tokens), F32),
            pltpu.VMEM((2 * RING, 2, tokens), F32),
            buf(N_OFF, 128, 128),
            buf(N_OFF, 128, 128),
            pltpu.VMEM((2, reach, 128), F32),
            buf(2 * RING, tokens, 128),
            dma((12,)),
            dma((RING, 3)),
            *both(len(FAR)),
            *both(FAR_AT),
            *both(FAR_AT),
            *both(4, 2),
            *both(4, 2),
            *both(RING, 2),
            *both(RING, 3),
            *both(4, 3),
            *both(4, 3),
            *both(N_OFF),
            *both(4, 2),
            *both(4, 2),
            *both(RING, 2),
            *both(2 * RING),
            *both(N_OFF),
            *both(1),
        ],
        compiler_params=pltpu.CompilerParams(
            collective_id=0, has_side_effects=True, vmem_limit_bytes=60 << 20
        ),
        name="experts",
    )(
        ids, weight, rows_in, cotangent, w_gate, w_up, w_down, w_out, gain, conv_out, mean, rstd
    )


def on_device(
    saved_input,
    cotangent,
    expert_ids,
    route_weight,
    w_gate,
    w_up,
    w_down,
    w_out,
    channel_gain,
    conv_taps,
    glu_value,
    glu_gate,
    conv_out,
    norm_mean,
    norm_rstd,
):
    reach = 32
    parts = experts(
        expert_ids.T,
        route_weight.T,
        saved_input,
        cotangent,
        w_gate[0],
        w_up[0],
        w_down[0],
        w_out,
        channel_gain[None],
        conv_out,
        norm_mean[None],
        norm_rstd[None],
        reach,
    )
    gate_grad, up_grad, down_grad, proj_grad, value_grad, gate_in_grad = finish(
        *parts, conv_taps, glu_value, glu_gate
    )
    return (
        gate_grad[None],
        up_grad[None],
        down_grad[None],
        proj_grad,
        value_grad,
        gate_in_grad,
    )


def solution(mesh):
    in_specs = (
        P("sp", None),
        P("sp", None),
        P("sp", None),
        P("sp", None),
        P("sp", None, "tp"),
        P("sp", None, "tp"),
        P("sp", "tp", None),
        P(None, "tp"),
        P("tp"),
        P(None, "tp"),
        P("tp", "sp"),
        P("tp", "sp"),
        P("tp", "sp"),
        P("sp"),
        P("sp"),
    )
    out_specs = (
        P("sp", None, "tp"),
        P("sp", None, "tp"),
        P("sp", "tp", None),
        P("sp", "tp"),
        P("tp", "sp"),
        P("tp", "sp"),
    )
    return jax.shard_map(
        on_device, mesh=mesh, in_specs=in_specs, out_specs=out_specs, check_vma=False
    )
```

```python
import jax
import jax.numpy as jnp
from jax import lax
from jax.experimental import pallas as pl
from jax.experimental.pallas import tpu as pltpu
from jax.sharding import PartitionSpec as P

D = 2048
C = 2048
HIDDEN = 384
SIDE = 4
RING = 8
CAP = 64
BF16 = jnp.bfloat16
F32 = jnp.float32
MESH = pl.DeviceIdType.MESH

NEXT = ((0, 1), (0, 3), (1, 0), (3, 0))
CORNER = ((1, 1), (3, 3), (1, 3), (3, 1))
HERE = ((0, 0),)
ACROSS = ((0, 2), (2, 0))
FAR = ((1, 2), (3, 2), (2, 1), (2, 3), (2, 2))
OFFSETS = NEXT + ACROSS + HERE + CORNER + FAR
N_OFF = len(OFFSETS)
LOCAL = OFFSETS.index((0, 0))
FAR_AT = N_OFF - len(FAR)
HALVES = ((0, 3), (3, 2))
ROWS = N_OFF * CAP
SPANS = ((0, 7 * CAP), (7 * CAP, 4 * CAP), (11 * CAP, 5 * CAP))


def sp_at(dy, dx):
    sp = lax.axis_index("sp")
    y, x = sp // SIDE, sp % SIDE
    return ((y + dy) % SIDE) * SIDE + (x + dx) % SIDE


def contract(left, right, left_dim, right_dim):
    return lax.dot_general(
        left, right, (((left_dim,), (right_dim,)), ((), ())), preferred_element_type=F32
    )


class Copies:
    def __init__(self):
        self.started = []

    def send(self, src, dst, sems, at, device):
        copy = pltpu.make_async_remote_copy(
            src_ref=src,
            dst_ref=dst,
            send_sem=sems[0].at[at],
            recv_sem=sems[1].at[at],
            device_id=device,
            device_id_type=MESH,
        )
        copy.start()
        self.started.append(copy)

    def arrived(self, dst, sems, at, device):
        pltpu.make_async_remote_copy(
            src_ref=dst,
            dst_ref=dst,
            send_sem=sems[0].at[at],
            recv_sem=sems[1].at[at],
            device_id=device,
            device_id_type=MESH,
        ).wait_recv()

    def finish(self):
        for copy in self.started:
            copy.wait_send()


def spread_ring(copies, block, source, core, z, up, down, partner, ups, downs, shares, between):
    def spread(src, g, k, half, going_up, going_down, slot):
        dst = block(g, core, half)
        if going_up:
            copies.send(src, dst, ups, (k, half), up)
        if going_down:
            copies.send(src, dst, downs, (k, half), down)
        copies.send(src, dst, shares, (slot, half), partner)

    for half in range(2):
        spread(source(half), z, 0, half, True, True, 0)
    between(0)
    for k in range(1, 5):
        above, below = (z + RING - k) % RING, (z + k) % RING
        for half in range(2):
            if k < 4 or half == 0:
                here = block(above, core, half)
                copies.arrived(here, ups, (k - 1, half), up)
                spread(here, above, k, half, k < 3 or (k == 3 and half == 0), False, k)
            if k < 4 or half == 1:
                here = block(below, core, half)
                copies.arrived(here, downs, (k - 1, half), down)
                spread(
                    here,
                    below,
                    k,
                    half,
                    False,
                    k < 3 or (k == 3 and half == 1),
                    4 if k == 4 else 4 + k,
                )
        between(k)
    for slot in range(RING):
        g = (z + RING - slot) % RING if slot <= 4 else (z + slot - 4) % RING
        for half in range(2):
            copies.arrived(block(g, 1 - core, half), shares, (slot, half), partner)


def experts_kernel(
    ids_in,
    weight_in,
    rows_in_ref,
    cot_in,
    wg_ref,
    wu_ref,
    wd_ref,
    wo_in,
    gain_in,
    conv_in,
    mean_in,
    rstd_in,
    gg_out,
    ug_out,
    dg_out,
    cc_ref,
    proj_ref,
    ids_ref,
    weight_ref,
    in_ref,
    cot_ref,
    wo_ref,
    gain_ref,
    conv_ref,
    mean_ref,
    rstd_ref,
    gg_ref,
    ug_ref,
    dg_ref,
    m_ref,
    src0,
    src1,
    x_far,
    x_near,
    r,
    wgu,
    wd,
    gu,
    hid,
    hid_t,
    p,
    pair_buf,
    out_up,
    in_up,
    out_down,
    in_down,
    sums,
    slots,
    chosen,
    mixed,
    act,
    factor,
    centered,
    total_out,
    total_in,
    proj_out,
    proj_in,
    rim,
    blocks,
    *sems,
):
    (load_sem, grad_sem, *pairs) = sems
    firsts = [
        pltpu.make_async_copy(src, dst, load_sem.at[3 + i])
        for i, (src, dst) in enumerate(
            (
                (ids_in, ids_ref),
                (weight_in, weight_ref),
                (cot_in, cot_ref),
                (rows_in_ref, in_ref),
                (conv_in, conv_ref),
                (mean_in, mean_ref),
                (rstd_in, rstd_ref),
                (gain_in, gain_ref),
                (wo_in, wo_ref),
            )
        )
    ]
    for first in firsts:
        first.start()
    grads = []
    (far_s, near_s, nshare_s, up_s, down_s, share_s, pair_s) = [
        (pairs[2 * i], pairs[2 * i + 1]) for i in range(7)
    ]
    (rup_s, rdown_s, back_s, gup_s, gdown_s, gshare_s, total_s, proj_s, rim_s) = [
        (pairs[2 * i], pairs[2 * i + 1]) for i in range(7, 16)
    ]
    sp, tp = lax.axis_index("sp"), lax.axis_index("tp")
    y, x = sp // SIDE, sp % SIDE
    z, core = tp // 2, tp % 2
    partner = (sp, z * 2 + 1 - core)
    up = (sp, ((z + 1) % RING) * 2 + core)
    down = (sp, ((z + RING - 1) % RING) * 2 + core)
    n_tp = 2 * RING
    others = [(sp, (tp + d) % n_tp) for d in range(1, n_tp)]
    others += [(sp_at(dy, dx), tp) for dy, dx in OFFSETS if (dy, dx) != (0, 0)]
    barrier = pltpu.get_barrier_semaphore()
    for device in others:
        pl.semaphore_signal(barrier, inc=1, device_id=device, device_id_type=MESH)
    copies = Copies()
    tokens = in_ref.shape[0]

    loads = [
        pltpu.make_async_copy(wg_ref, wgu.at[:, pl.ds(0, HIDDEN)], load_sem.at[0]),
        pltpu.make_async_copy(wu_ref, wgu.at[:, pl.ds(HIDDEN, HIDDEN)], load_sem.at[1]),
        pltpu.make_async_copy(wd_ref, wd, load_sem.at[2]),
    ]
    for load in loads:
        load.start()

    for first in firsts[:2]:
        first.wait()
    n_experts = N_OFF
    expert = lax.broadcasted_iota(jnp.int32, (n_experts, tokens), 0)
    one = [(ids_ref[k : k + 1, :] == expert).astype(F32) for k in range(2)]
    earlier = (
        lax.broadcasted_iota(jnp.int32, (tokens, tokens), 0)
        < lax.broadcasted_iota(jnp.int32, (tokens, tokens), 1)
    ).astype(BF16)
    before = jnp.dot((one[0] + one[1]).astype(BF16), earlier, preferred_element_type=F32)
    place = jnp.zeros((n_experts, tokens), jnp.int32)
    for o, (dy, dx) in enumerate(OFFSETS):
        place = jnp.where(
            expert == ((y + dy) % SIDE) * SIDE + (x + dx) % SIDE, o * CAP, place
        )
    row_of = before + place.astype(F32)
    row_f = [jnp.sum(one[k] * row_of, axis=0, keepdims=True) for k in range(2)]
    row = [value.astype(jnp.int32) for value in row_f]

    def column(value):
        return jnp.transpose(jnp.broadcast_to(value, (128, tokens)))

    for first in firsts[2:4]:
        first.wait()
    for k, src in enumerate((src0, src1)):
        scale = column(weight_ref[k : k + 1, :])
        for j in range(D // 128):
            part = pl.ds(j * 128, 128)
            scaled = (scale * cot_ref[:, part].astype(F32)).astype(BF16)
            src[:, part] = jnp.where(core == 0, in_ref[:, part], scaled)

    def picked(at):
        return (
            jnp.dot((row[0] == at).astype(BF16), src0[...], preferred_element_type=F32)
            + jnp.dot((row[1] == at).astype(BF16), src1[...], preferred_element_type=F32)
        ).astype(BF16)

    def fill(first, count):
        at = lax.broadcasted_iota(jnp.int32, (count * CAP, tokens), 0) + first * CAP
        x_near[pl.ds(first, count)] = picked(at).reshape(count, RING, 8, D)

    def send_near(first, count):
        for o in range(first, first + count):
            if o == LOCAL:
                copies.send(x_near.at[o], r.at[core, o], nshare_s, o, partner)
            else:
                copies.send(
                    x_near.at[o], r.at[core, o], near_s, o, (sp_at(*OFFSETS[o]), tp)
                )

    index = lax.broadcasted_iota(jnp.int32, (len(FAR) * 8, tokens), 0)
    x_far[...] = picked((FAR_AT + index // 8) * CAP + z * 8 + index % 8).reshape(len(FAR), 8, D)
    fill(0, 4)
    pl.semaphore_wait(barrier, len(others))
    for i, offset in enumerate(FAR):
        copies.send(
            x_far.at[i], r.at[core, FAR_AT + i, z], far_s, i, (sp_at(*offset), tp)
        )
    fill(4, 3)
    send_near(0, 4)
    fill(7, 4)
    send_near(4, 3)
    send_near(7, 4)
    r[core, LOCAL] = x_near[LOCAL]

    def prepare():
        for first in firsts[4:]:
            first.wait()
        gain = gain_ref[...]
        rstd = column(rstd_ref[...])
        cent = (jnp.transpose(conv_ref[...].astype(F32)) - column(mean_ref[...])) * rstd
        normed = cent * gain
        sigma = jax.nn.sigmoid(normed)
        centered[...] = cent
        factor[...] = sigma * (1.0 + normed * (1.0 - sigma)) * gain
        act[...] = jnp.transpose(normed * sigma).astype(BF16)
        where = [column(value).astype(jnp.int32) for value in row_f]
        for j in range(ROWS // 128):
            at = lax.broadcasted_iota(jnp.int32, (tokens, 128), 1) + j * 128
            chosen[:, pl.ds(j * 128, 128)] = ((where[0] == at) | (where[1] == at)).astype(BF16)

    def far(g, c, half):
        start, size = HALVES[half]
        return r.at[c, pl.ds(FAR_AT + start, size), g]

    def forward(first, count):
        for o in range(first, first + count):
            if o != LOCAL:
                copies.arrived(r.at[core, o], near_s, o, partner)
                copies.send(r.at[core, o], r.at[core, o], nshare_s, o, partner)

    def shared(first, count):
        for o in range(first, first + count):
            copies.arrived(r.at[1 - core, o], nshare_s, o, partner)

    def forward_group(first, count):
        span = pl.ds(first * CAP, count * CAP)
        rows_in = r[0, pl.ds(first, count)].reshape(count * CAP, D)
        rows_cot = r[1, pl.ds(first, count)].reshape(count * CAP, D)
        both = jnp.dot(rows_in, wgu[...], preferred_element_type=F32)
        gate_pre, up_pre = both[:, :HIDDEN], both[:, HIDDEN:]
        hidden_cot = contract(rows_cot, wd[...], 1, 1)
        sigma = jax.nn.sigmoid(gate_pre)
        hid[span, :] = (gate_pre * sigma * up_pre).astype(BF16)
        gu[span, pl.ds(0, HIDDEN)] = (
            hidden_cot * up_pre * sigma * (1.0 + gate_pre * (1.0 - sigma))
        ).astype(BF16)
        gu[span, pl.ds(HIDDEN, HIDDEN)] = (hidden_cot * gate_pre * sigma).astype(BF16)

    def at_z(d):
        return (z + RING + d) % RING

    def span(half):
        return pl.ds(*SPANS[half])

    def chunk(d, half):
        g = at_z(d)
        total = contract(
            gu[span(half), :], wgu[pl.ds(pl.multiple_of(g * 256, 256), 256), :], 1, 1
        ).astype(BF16)
        p[0, g, span(half), :] = total[:, :128]
        p[1, g, span(half), :] = total[:, 128:]
        copies.send(
            p.at[1 - core, g, span(half)],
            pair_buf.at[g, span(half)],
            pair_s,
            (d % RING, half),
            partner,
        )

    def own(d, half):
        g = at_z(d)
        copies.arrived(pair_buf.at[g, span(half)], pair_s, (d % RING, half), partner)
        return p[core, g, span(half), :].astype(F32) + pair_buf[g, span(half), :].astype(F32)

    def came(buf, sem, hop, half):
        copies.arrived(buf.at[hop, span(half)], sem, (hop, half), partner)
        return buf[hop, span(half), :].astype(F32)

    def step_up(hop, half):
        total = own(4 - hop, half)
        if hop > min(half, 1):
            total = total + came(in_up, rup_s, hop - 1, half)
        out_up[hop, span(half), :] = total.astype(BF16)

    def step_down(hop, half):
        total = own(hop - 4, half)
        if hop > 1 - min(half, 1):
            total = total + came(in_down, rdown_s, hop - 1, half)
        out_down[hop, span(half), :] = total.astype(BF16)

    def go_up(hop, half):
        here = (hop, span(half))
        copies.send(out_up.at[here], in_up.at[here], rup_s, (hop, half), up)

    def go_down(hop, half):
        here = (hop, span(half))
        copies.send(out_down.at[here], in_down.at[here], rdown_s, (hop, half), down)

    def weight_grads(i):
        part = pl.ds(i * 256, 256)
        rows_in = r[0, :, :, :, part].reshape(ROWS, 256)
        rows_cot = r[1, :, :, :, part].reshape(ROWS, 256)
        both = contract(rows_in, gu[...], 0, 0).astype(BF16)
        gg_ref[part, :] = both[:, :HIDDEN]
        ug_ref[part, :] = both[:, HIDDEN:]
        dg_ref[:, part] = jnp.dot(hid_t[...], rows_cot, preferred_element_type=F32).astype(BF16)
        for j, (buf, out, at) in enumerate(
            ((gg_ref, gg_out, part), (ug_ref, ug_out, part), (dg_ref, dg_out, (slice(None), part)))
        ):
            grads.append(pltpu.make_async_copy(buf.at[at], out.at[at], grad_sem.at[i, j]))
            grads[-1].start()

    def between(k):
        if k == 0:
            prepare()
            for load in loads:
                load.wait()
        if k == 1:
            forward(0, 4)
        if k == 2:
            shared(0, 4)
            forward_group(0, 4)
        if k == 3:
            forward(4, 3)
            shared(4, 3)
            forward_group(4, 3)
            chunk(4, 0)
            chunk(-3, 0)
            step_up(0, 0)
            go_up(0, 0)
            step_down(1, 0)
            go_down(1, 0)
        if k == 4:
            chunk(3, 0)
            chunk(-2, 0)
            step_up(1, 0)
            go_up(1, 0)
            step_down(2, 0)
            go_down(2, 0)
            chunk(2, 0)
            chunk(-1, 0)
            chunk(1, 0)
            forward(7, 4)
            shared(7, 4)
            forward_group(7, 4)
            chunk(4, 1)
            chunk(3, 1)
            step_down(0, 1)
            go_down(0, 1)
            step_up(1, 1)
            go_up(1, 1)

    def hop_on(ups, downs):
        for hop, half in ups:
            step_up(hop, half)
            go_up(hop, half)
        for hop, half in downs:
            step_down(hop, half)
            go_down(hop, half)

    for i in range(len(FAR)):
        copies.arrived(r.at[core, FAR_AT + i, z], far_s, i, partner)
    spread_ring(
        copies,
        far,
        lambda half: far(z, core, half),
        core,
        z,
        up,
        down,
        partner,
        up_s,
        down_s,
        share_s,
        between,
    )
    forward_group(FAR_AT, len(FAR))
    chunk(4, 2)
    chunk(3, 2)
    hop_on(((1, 2),), ((0, 2),))
    hop_on(((2, 0),), ((3, 0),))
    chunk(-3, 1)
    chunk(2, 1)
    hop_on(((2, 1),), ((1, 1),))
    chunk(-3, 2)
    chunk(2, 2)
    hop_on(((2, 2),), ((1, 2),))
    hop_on(((3, 0),), ())
    chunk(-2, 1)
    chunk(1, 1)
    hop_on(((3, 1),), ((2, 1),))
    chunk(-2, 2)
    chunk(1, 2)
    hop_on(((3, 2),), ((2, 2),))
    chunk(-1, 1)
    chunk(-1, 2)
    hid_t[...] = jnp.transpose(hid[...])
    weight_grads(0)
    hop_on((), ((3, 1),))
    hop_on((), ((3, 2),))
    for half in range(3):
        chunk(0, half)
    weight_grads(1)
    weight_grads(2)
    for half in range(3):
        sums[span(half), :] = (
            own(0, half) + came(in_up, rup_s, 3, half) + came(in_down, rdown_s, 3, half)
        ).astype(BF16)
    for o in reversed(range(N_OFF)):
        if o != LOCAL:
            dy, dx = OFFSETS[o]
            part = pl.ds(o * CAP, CAP)
            copies.send(sums.at[part], slots.at[part], back_s, o, (sp_at(-dy, -dx), tp))
    here = pl.ds(LOCAL * CAP, CAP)
    slots[here, :] = sums[here, :]
    weight_grads(3)
    weight_grads(4)
    for o in range(N_OFF):
        if o != LOCAL:
            copies.arrived(slots.at[pl.ds(o * CAP, CAP)], back_s, o, partner)
    total = jnp.dot(chosen[...], slots[...], preferred_element_type=F32)
    mine = pl.ds(pl.multiple_of(tp * 128, 128), 128)
    mixed[...] = (cot_ref[:, mine].astype(F32) + total).astype(BF16)

    half_tokens = tokens // 2

    def block(g, c, half):
        return blocks.at[g * 2 + c, pl.ds(half * half_tokens, half_tokens)]

    def between_gather(k):
        if k == 0:
            blocks[tp] = mixed[...]
            weight_grads(5)

    spread_ring(
        copies,
        block,
        lambda half: mixed.at[pl.ds(half * half_tokens, half_tokens)],
        core,
        z,
        up,
        down,
        partner,
        gup_s,
        gdown_s,
        gshare_s,
        between_gather,
    )

    for j in range(n_tp):
        m_ref[:, pl.ds(j * 128, 128)] = blocks[j]
    for s in range(N_OFF // 4):
        part = jnp.dot(act[...], m_ref[:, pl.ds(s * 512, 512)], preferred_element_type=F32)
        for i in range(4):
            proj_out[4 * s + i] = part[:, i * 128 : i * 128 + 128].astype(BF16)
    for o in range(N_OFF):
        if o != LOCAL:
            peer = sp_at(*OFFSETS[o])
            copies.send(proj_out.at[peer], proj_in.at[o], proj_s, o, (peer, tp))
    proj_in[LOCAL] = proj_out[sp]
    act_cot = jnp.dot(m_ref[...], wo_ref[...], preferred_element_type=F32)
    norm_cot = act_cot * factor[...]
    for i, value in enumerate((norm_cot, norm_cot * centered[...])):
        whole = jnp.broadcast_to(jnp.sum(value, axis=1, keepdims=True), (tokens, 128))
        total_out[i : i + 1, :] = jnp.transpose(whole)[0:1, :]
    total_in[tp] = total_out[...]
    for d in range(1, n_tp):
        copies.send(total_out, total_in.at[tp], total_s, d, (sp, (tp + d) % n_tp))
    weight_grads(6)
    weight_grads(7)
    for d in range(1, n_tp):
        copies.arrived(total_in.at[(tp + n_tp - d) % n_tp], total_s, d, partner)
    totals = jnp.sum(total_in[...], axis=0)
    conv_cot = column(rstd_ref[...]) * (
        norm_cot - column(totals[0:1, :]) / C - centered[...] * (column(totals[1:2, :]) / C)
    )
    cc_ref[pl.ds(0, tokens), :] = conv_cot
    n_rim = rim.shape[1]
    rim[0] = conv_cot[:n_rim, :]
    copies.send(rim.at[0], rim.at[1], rim_s, 0, ((sp + N_OFF - 1) % N_OFF, tp))
    for o in range(N_OFF):
        if o != LOCAL:
            copies.arrived(proj_in.at[o], proj_s, o, partner)
    proj_ref[...] = jnp.sum(proj_in[...].astype(F32), axis=0)
    copies.arrived(rim.at[1], rim_s, 0, partner)
    cc_ref[pl.ds(tokens, n_rim), :] = jnp.where(sp == N_OFF - 1, 0.0, rim[1])
    for grad in grads:
        grad.wait()
    copies.finish()


def finish_kernel(
    gg_ref,
    ug_ref,
    dg_ref,
    cc_ref,
    proj_ref,
    taps_ref,
    value_ref,
    gate_ref,
    gg_out,
    ug_out,
    dg_out,
    proj_out,
    value_out,
    gate_out,
    gg,
    ug,
    dg,
    in_sem,
    out_sem,
):
    takes, gives = [], []
    for i, (src, buf, dst) in enumerate(
        ((gg_ref, gg, gg_out), (ug_ref, ug, ug_out), (dg_ref, dg, dg_out))
    ):
        size = src.shape[0] // 2
        for j in range(2):
            part = pl.ds(j * size, size)
            takes.append(pltpu.make_async_copy(src.at[part], buf.at[part], in_sem.at[i, j]))
            gives.append(pltpu.make_async_copy(buf.at[part], dst.at[part], out_sem.at[i, j]))
    for take in takes:
        take.start()
    tokens = value_ref.shape[1]
    total = taps_ref[0:1, :] * cc_ref[pl.ds(0, tokens), :]
    for lag in range(1, taps_ref.shape[0]):
        total = total + taps_ref[lag : lag + 1, :] * cc_ref[pl.ds(lag, tokens), :]
    for take, give in zip(takes, gives):
        take.wait()
        give.start()
    glu_cot = jnp.transpose(total)
    sigma = jax.nn.sigmoid(gate_ref[...].astype(F32))
    value_out[...] = (glu_cot * sigma).astype(BF16)
    gate_out[...] = (glu_cot * value_ref[...].astype(F32) * sigma * (1.0 - sigma)).astype(BF16)
    proj_out[...] = jnp.transpose(proj_ref[...])
    for give in gives:
        give.wait()


def finish(gg, ug, dg, cc, proj, taps, value, gate):
    vmem = pl.BlockSpec(memory_space=pltpu.VMEM)
    anywhere = pl.BlockSpec(memory_space=pl.ANY)

    def like(a):
        return jax.ShapeDtypeStruct(a.shape, a.dtype)

    return pl.pallas_call(
        finish_kernel,
        out_shape=(like(gg), like(ug), like(dg), like(proj), like(value), like(value)),
        in_specs=[anywhere] * 3 + [vmem] * 5,
        out_specs=(anywhere,) * 3 + (vmem,) * 3,
        scratch_shapes=[
            *[pltpu.VMEM(a.shape, a.dtype) for a in (gg, ug, dg)],
            pltpu.SemaphoreType.DMA((3, 2)),
            pltpu.SemaphoreType.DMA((3, 2)),
        ],
        compiler_params=pltpu.CompilerParams(vmem_limit_bytes=60 << 20),
        name="finish",
    )(gg, ug, dg, cc, proj, taps, value, gate)


def experts(
    ids, weight, rows_in, cotangent, w_gate, w_up, w_down, w_out, gain, conv_out, mean, rstd, reach
):
    dma = pltpu.SemaphoreType.DMA
    tokens = cotangent.shape[0]
    vmem = pl.BlockSpec(memory_space=pltpu.VMEM)
    anywhere = pl.BlockSpec(memory_space=pl.ANY)

    def both(*shape):
        return [dma(shape), dma(shape)]

    def buf(*shape):
        return pltpu.VMEM(shape, BF16)

    return pl.pallas_call(
        experts_kernel,
        out_shape=(
            jax.ShapeDtypeStruct((D, HIDDEN), BF16),
            jax.ShapeDtypeStruct((D, HIDDEN), BF16),
            jax.ShapeDtypeStruct((HIDDEN, D), BF16),
            jax.ShapeDtypeStruct((tokens + reach, 128), F32),
            jax.ShapeDtypeStruct((128, 128), F32),
        ),
        in_specs=[anywhere] * 12,
        out_specs=(anywhere,) * 3 + (vmem,) * 2,
        scratch_shapes=[
            *[pltpu.VMEM(a.shape, a.dtype) for a in (ids, weight, rows_in, cotangent)],
            *[pltpu.VMEM(a.shape, a.dtype) for a in (w_out, gain, conv_out, mean, rstd)],
            buf(D, HIDDEN),
            buf(D, HIDDEN),
            buf(HIDDEN, D),
            buf(tokens, D),
            buf(tokens, D),
            buf(tokens, D),
            buf(len(FAR), 8, D),
            buf(FAR_AT, RING, 8, D),
            buf(2, N_OFF, RING, 8, D),
            buf(D, 2 * HIDDEN),
            buf(HIDDEN, D),
            buf(ROWS, 2 * HIDDEN),
            buf(ROWS, HIDDEN),
            buf(HIDDEN, ROWS),
            buf(2, RING, ROWS, 128),
            buf(RING, ROWS, 128),
            buf(4, ROWS, 128),
            buf(4, ROWS, 128),
            buf(4, ROWS, 128),
            buf(4, ROWS, 128),
            buf(ROWS, 128),
            buf(ROWS, 128),
            buf(tokens, ROWS),
            buf(tokens, 128),
            buf(128, tokens),
            pltpu.VMEM((tokens, 128), F32),
            pltpu.VMEM((tokens, 128), F32),
            pltpu.VMEM((2, tokens), F32),
            pltpu.VMEM((2 * RING, 2, tokens), F32),
            buf(N_OFF, 128, 128),
            buf(N_OFF, 128, 128),
            pltpu.VMEM((2, reach, 128), F32),
            buf(2 * RING, tokens, 128),
            dma((12,)),
            dma((RING, 3)),
            *both(len(FAR)),
            *both(FAR_AT),
            *both(FAR_AT),
            *both(4, 2),
            *both(4, 2),
            *both(RING, 2),
            *both(RING, 3),
            *both(4, 3),
            *both(4, 3),
            *both(N_OFF),
            *both(4, 2),
            *both(4, 2),
            *both(RING, 2),
            *both(2 * RING),
            *both(N_OFF),
            *both(1),
        ],
        compiler_params=pltpu.CompilerParams(
            collective_id=0, has_side_effects=True, vmem_limit_bytes=60 << 20
        ),
        name="experts",
    )(
        ids, weight, rows_in, cotangent, w_gate, w_up, w_down, w_out, gain, conv_out, mean, rstd
    )


def on_device(
    saved_input,
    cotangent,
    expert_ids,
    route_weight,
    w_gate,
    w_up,
    w_down,
    w_out,
    channel_gain,
    conv_taps,
    glu_value,
    glu_gate,
    conv_out,
    norm_mean,
    norm_rstd,
):
    reach = 32
    parts = experts(
        expert_ids.T,
        route_weight.T,
        saved_input,
        cotangent,
        w_gate[0],
        w_up[0],
        w_down[0],
        w_out,
        channel_gain[None],
        conv_out,
        norm_mean[None],
        norm_rstd[None],
        reach,
    )
    gate_grad, up_grad, down_grad, proj_grad, value_grad, gate_in_grad = finish(
        *parts, conv_taps, glu_value, glu_gate
    )
    return (
        gate_grad[None],
        up_grad[None],
        down_grad[None],
        proj_grad,
        value_grad,
        gate_in_grad,
    )


def solution(mesh):
    in_specs = (
        P("sp", None),
        P("sp", None),
        P("sp", None),
        P("sp", None),
        P("sp", None, "tp"),
        P("sp", None, "tp"),
        P("sp", "tp", None),
        P(None, "tp"),
        P("tp"),
        P(None, "tp"),
        P("tp", "sp"),
        P("tp", "sp"),
        P("tp", "sp"),
        P("sp"),
        P("sp"),
    )
    out_specs = (
        P("sp", None, "tp"),
        P("sp", None, "tp"),
        P("sp", "tp", None),
        P("sp", "tp"),
        P("tp", "sp"),
        P("tp", "sp"),
    )
    return jax.shard_map(
        on_device, mesh=mesh, in_specs=in_specs, out_specs=out_specs, check_vma=False
    )
```
